256 devices in a mesh: ep: 128 (over z, y, x), tp: 2 (over core).
Axes of the slice: x: 4, y: 4, z: 8, core: 2. Of those that a mesh axis runs over, the one named last changes fastest.
Arguments:
- resid: bfloat16 [2048, 2048], P('ep'), may hold values from -6 to 6
- proj_x: bfloat16 [2048, 2048], P('ep', 'tp'), may hold values from -6 to 6
- proj_z: bfloat16 [2048, 2048], P('ep', 'tp'), may hold values from -6 to 6
- proj_bc: bfloat16 [2048, 2, 512], P('ep', None, 'tp'), may hold values from -6 to 6
- proj_dt: bfloat16 [2048, 32], P('ep', 'tp'), may hold values from -6 to 6
- tail_x: bfloat16 [2048, 3, 2048], P('ep', None, 'tp'), may hold values from -6 to 6
- tail_bc: bfloat16 [2048, 3, 2, 512], P('ep', None, None, 'tp'), may hold values from -6 to 6
- taps_x: bfloat16 [4, 2048], P(None, 'tp'), may hold values from -3 to 3
- taps_bc: bfloat16 [4, 2, 512], P(None, None, 'tp'), may hold values from -3 to 3
- ssm_state: float32 [2048, 32, 4096], P('ep', 'tp'), may hold values from -1.5 to 1.5
- dt_bias: float32 [32], P('tp'), may hold values from -4 to 0
- decay_log: float32 [32], P('tp'), may hold values from -1 to 2.5
- group_gain: float32 [2048], P('tp'), may hold values from 0.1 to 1.9
- out_proj: bfloat16 [2048, 2048], P('tp', 'ep'), may hold values from -0.125 to 0.125
- ffn_gain: float32 [2048], replicated, may hold values from 0.1 to 1.9
- dense_gate: bfloat16 [2048, 4096], P(None, ('ep', 'tp')), may hold values from -0.125 to 0.125
- dense_up: bfloat16 [2048, 4096], P(None, ('ep', 'tp')), may hold values from -0.125 to 0.125
- dense_down: bfloat16 [4096, 2048], P(('ep', 'tp')), may hold values from -0.09375 to 0.09375
- branch_gate: bfloat16 [2048], replicated, may hold values from -0.125 to 0.125
- group_weights: float32 [2048, 4], replicated, may hold values from 0.2 to 1
- expert_ids: int32 [2048, 6], replicated, may hold values from 0 to 127, all different within a row; in each aligned block of 16 rows (0 to 15, 16 to 31, ...) at most 2 rows name the same one
- expert_weights: float32 [2048, 6], replicated, may hold values from 0.1 to 1
- exp_gate: bfloat16 [128, 2048, 512], P('ep', None, 'tp'), may hold values from -0.125 to 0.125
- exp_up: bfloat16 [128, 2048, 512], P('ep', None, 'tp'), may hold values from -0.125 to 0.125
- exp_down: bfloat16 [128, 512, 2048], P('ep', 'tp'), may hold values from -0.25 to 0.25
Outputs:
- out: bfloat16 [2048, 2048], P(('ep', 'tp'))
- new_state: float32 [2048, 32, 4096], P('ep', 'tp')
The draws below stay inside these ranges and needn't reach their ends.
Inputs may be any that keep to these rules, and one draw needn't show every extreme that they name: `expert_ids`: each row names 6 different experts. In the rows of one index of ep (aligned blocks of 16 rows) no expert is named more than 2 times, a bound that some block reaches.
All inputs are finite; a program needn't handle non-finite values.
Results may differ from the reference program's by a relative error of at most 0.013.
Values may be sent and summed in bfloat16 or wider, within the bound.
A program may use at most 128 MiB of HBM per device.

```python
import math
import jax
import jax.numpy as jnp
import numpy as np
from jax import lax

D = 2048
HEADS = 32
HEAD_P = 64
NSTATE = 64
BC_GROUPS = 8
TAPS = 4
EFF = 512
DFF = 4096
GROUPS = 4
TOPK = 6
SEQ_DEV = 16
INNER = 2048
HPG = 4
BATCH = 2048
EXPERTS = 128
EPG = 32
CAP = 2


def block_scale(own_key, dims, shards, smallest, largest):
    gain, own = 1.0, jax.random.fold_in(own_key, 6)
    for dim, parts in shards:
        steps = jnp.exp(jax.random.uniform(jax.random.fold_in(own, dim), (parts,), jnp.float32, smallest / len(shards), largest / len(shards)))
        gain = gain * jnp.repeat(steps, dims[dim] // parts).reshape([-1 if axis == dim else 1 for axis in range(len(dims))])
    return gain


def shared_out(own_key, own, number, rows, count, top, most, slope):
    sequence = jax.random.permutation(own_key, count)
    crowded, common = portions_of(count, rows * top, most, slope, True), portions_of(count, rows * top, most, slope, False)
    places = jnp.arange(count)

    def named(lengths, offset_by):
        used = int((lengths > 0).sum())
        fixed = max(1, used // 4)
        shifted = fixed + (places - fixed + offset_by * (used - fixed)) % max(1, count - fixed)
        return jnp.zeros((count,), jnp.int32).at[sequence[jnp.where(places < fixed, places, shifted)]].set(jnp.asarray(lengths, jnp.int32))

    lengths = jnp.where(number % 4 == 0, named(crowded, number // 4), named(common, number - number // 4 - 1))
    mixed = jax.random.permutation(jax.random.fold_in(own, 3), count)
    donor, receiver = mixed[0:count // 2 * 2:2], mixed[1:count // 2 * 2:2]
    room = jnp.minimum(lengths[donor] - 1, most - lengths[receiver]) // 2
    room = jnp.where((donor == sequence[0]) | (receiver == sequence[0]) | (lengths[receiver] == 0), 0, jnp.maximum(room, 0))
    shifted = jax.random.randint(jax.random.fold_in(own, 4), (count // 2,), 0, 1 << 20) % (room + 1)
    lengths = lengths.at[donor].add(-shifted).at[receiver].add(shifted)
    members = jnp.searchsorted(jnp.cumsum(lengths), jnp.arange(rows * top), side="right").astype(jnp.int32)
    table = members.reshape(top, rows).T
    table = table[jax.random.permutation(jax.random.fold_in(own, 1), rows)]
    offset_by = jax.random.randint(jax.random.fold_in(own, 2), (rows, 1), 0, top)
    return jnp.take_along_axis(table, (jnp.arange(top)[None, :] + offset_by) % top, axis=1)


def portions_of(count, total, limit, lean, full):
    loads = [(1 << 20) // math.isqrt(standing ** lean) + 1 for standing in range(1, count + 1)]
    largest = limit if full else min(limit, max(-(-total // count), total * loads[0] // sum(loads)))
    least = 1 if total - largest >= count - 1 else 0
    holding, rest = [largest] + [least] * (count - 1), total - largest - least * (count - 1)
    while rest > 0:
        free = [i for i in range(1, count) if holding[i] < largest] or [i for i in range(1, count) if holding[i] < limit]
        whole, left = sum([loads[i] for i in free]), rest
        for i in free:
            addition = min(limit - holding[i], max(1, left * loads[i] // whole), rest)
            holding[i] = holding[i] + addition
            rest = rest - addition
    return np.array(holding)


def gaussian(stream_key, dims, scale, most, cuts=(), kind=jnp.bfloat16):
    drawn = jax.random.normal(stream_key, dims, jnp.float32) * scale
    if len(cuts) > 0:
        drawn = block_scale(stream_key, dims, cuts, -0.22, 0.18) * drawn
    return jnp.clip(drawn, min=-most, max=most).astype(kind)


def setup_inputs(seed: int = 0) -> dict:
    key_of = jax.random.split(jax.random.key(seed), 26)
    resid = gaussian(key_of[0], (BATCH, D), 1.0, 6.0, ((0, 128),))
    proj_x = gaussian(key_of[1], (BATCH, INNER), 1.0, 6.0, ((0, 128), (1, 2)))
    proj_z = gaussian(key_of[2], (BATCH, INNER), 1.0, 6.0, ((0, 128), (1, 2)))
    proj_bc = gaussian(key_of[3], (BATCH, 2, BC_GROUPS * NSTATE), 1.0, 6.0, ((0, 128), (2, 2)))
    proj_dt = gaussian(key_of[4], (BATCH, HEADS), 1.0, 6.0, ((0, 128), (1, 2)))
    tail_x = gaussian(key_of[5], (BATCH, TAPS - 1, INNER), 1.0, 6.0, ((0, 128), (2, 2)))
    tail_bc = gaussian(key_of[6], (BATCH, TAPS - 1, 2, BC_GROUPS * NSTATE), 1.0, 6.0, ((0, 128), (3, 2)))
    taps_x = gaussian(key_of[7], (TAPS, INNER), TAPS ** -0.5, 3.0, ((1, 2),))
    taps_bc = gaussian(key_of[8], (TAPS, 2, BC_GROUPS * NSTATE), TAPS ** -0.5, 3.0, ((2, 2),))
    ssm_state = gaussian(key_of[9], (BATCH, HEADS, HEAD_P * NSTATE), 0.25, 1.5, ((0, 128), (1, 2)), jnp.float32)
    dt_bias = jnp.clip(-4.0 + 4.0 * jax.random.uniform(key_of[10], (HEADS,), jnp.float32) ** block_scale(key_of[10], (HEADS,), ((0, 2),), -0.2, 0.2), -4.0, 0.0)
    decay_log = jnp.clip(-1.0 + 3.5 * jax.random.uniform(key_of[11], (HEADS,), jnp.float32) ** block_scale(key_of[11], (HEADS,), ((0, 2),), -0.2, 0.2), -1.0, 2.5)
    group_gain = jnp.clip(1.0 + 0.18 * jax.random.normal(key_of[12], (INNER,), jnp.float32), 0.1, 1.9)
    out_proj = gaussian(key_of[13], (INNER, D), INNER ** -0.5, 0.125, ((0, 2), (1, 128)))
    ffn_gain = jnp.clip(1.0 + 0.18 * jax.random.normal(key_of[14], (D,), jnp.float32), 0.1, 1.9)
    dense_gate = gaussian(key_of[15], (D, DFF), D ** -0.5, 0.125, ((1, 256),))
    dense_up = gaussian(key_of[16], (D, DFF), D ** -0.5, 0.125, ((1, 256),))
    dense_down = gaussian(key_of[17], (DFF, D), DFF ** -0.5, 0.09375, ((0, 256),))
    branch_gate = gaussian(key_of[18], (D,), D ** -0.5, 0.125)
    group_weights = jnp.clip(jnp.exp(jax.random.uniform(key_of[19], (BATCH, GROUPS), jnp.float32, math.log(0.2), math.log(1.0))), 0.2, 1.0)
    expert_ids_keys = jax.random.split(jax.random.fold_in(key_of[20], 1), BATCH // SEQ_DEV)
    expert_ids_turns = jax.random.permutation(jax.random.fold_in(key_of[20], 3), BATCH // SEQ_DEV)
    expert_ids = jax.vmap(lambda own, number: shared_out(jax.random.fold_in(key_of[20], 2), own, number, SEQ_DEV, EXPERTS, TOPK, CAP, 2))(expert_ids_keys, expert_ids_turns).reshape((BATCH, TOPK))
    expert_weights = jnp.clip(jnp.exp(jax.random.uniform(key_of[21], (BATCH, TOPK), jnp.float32, math.log(0.1), math.log(1.0))), 0.1, 1.0)
    exp_gate = gaussian(key_of[22], (EXPERTS, D, EFF), D ** -0.5, 0.125, ((0, 128), (2, 2)))
    exp_up = gaussian(key_of[23], (EXPERTS, D, EFF), D ** -0.5, 0.125, ((0, 128), (2, 2)))
    exp_down = gaussian(key_of[24], (EXPERTS, EFF, D), EFF ** -0.5, 0.25, ((0, 128), (1, 2)))
    return {"resid": resid, "proj_x": proj_x, "proj_z": proj_z, "proj_bc": proj_bc, "proj_dt": proj_dt, "tail_x": tail_x, "tail_bc": tail_bc, "taps_x": taps_x, "taps_bc": taps_bc, "ssm_state": ssm_state, "dt_bias": dt_bias, "decay_log": decay_log, "group_gain": group_gain, "out_proj": out_proj, "ffn_gain": ffn_gain, "dense_gate": dense_gate, "dense_up": dense_up, "dense_down": dense_down, "branch_gate": branch_gate, "group_weights": group_weights, "expert_ids": expert_ids, "expert_weights": expert_weights, "exp_gate": exp_gate, "exp_up": exp_up, "exp_down": exp_down}


EPSILON = 1e-06

def state_update(proj_x, proj_z, proj_bc, proj_dt, tail_x, tail_bc, taps_x, taps_bc, ssm_state, dt_bias, decay_log, group_gain):
    window_x = jnp.concatenate([tail_x, proj_x[:, None]], axis=1).astype(jnp.float32)
    conv_x = jax.nn.silu(lax.optimization_barrier(jnp.sum(window_x * taps_x.astype(jnp.float32)[None], axis=1)))
    window_bc = jnp.concatenate([tail_bc, proj_bc[:, None]], axis=1).astype(jnp.float32)
    conv_bc = jax.nn.silu(lax.optimization_barrier(jnp.sum(window_bc * taps_bc.astype(jnp.float32)[None], axis=1)))
    count = proj_x.shape[0]
    heads = proj_dt.shape[1]
    x_heads = conv_x.reshape(count, heads, HEAD_P)
    grouped_bc = conv_bc.reshape(count, 2, heads // HPG, NSTATE)
    input_heads = jnp.repeat(grouped_bc[:, 0], HPG, axis=1)
    read_heads = jnp.repeat(grouped_bc[:, 1], HPG, axis=1)
    step_size = jax.nn.softplus(proj_dt.astype(jnp.float32) + dt_bias)
    decay = jnp.exp(-step_size * jnp.exp(decay_log))
    state = ssm_state.reshape(count, heads, HEAD_P, NSTATE)
    fresh = (step_size[:, :, None] * x_heads)[:, :, :, None] * input_heads[:, :, None, :]
    new_state = decay[:, :, None, None] * state + fresh
    readout = lax.optimization_barrier(jnp.sum(new_state * read_heads[:, :, None, :], axis=-1))
    gated = readout.reshape(count, heads * HEAD_P) * jax.nn.silu(proj_z.astype(jnp.float32))
    grouped = gated.reshape(count, heads // HPG, HPG * HEAD_P)
    grouped = grouped * lax.rsqrt(lax.optimization_barrier(jnp.mean(grouped * grouped, axis=-1, keepdims=True)) + EPSILON)
    y_out = (grouped.reshape(count, heads * HEAD_P) * group_gain).astype(jnp.bfloat16)
    return (y_out, new_state.reshape(count, heads, HEAD_P * NSTATE))

def expert_slots(expert_ids, expert_weights, group_weights, index, experts, group_size, capacity):
    batch = expert_ids.shape[0]
    rows_each = batch // experts
    pairs = rows_each * TOPK
    pick = (jnp.arange(GROUPS, dtype=jnp.int32) == index // group_size).astype(jnp.float32)
    coarse = lax.optimization_barrier(jnp.sum(group_weights * pick[None], axis=1))
    pair_weight = (expert_weights * coarse[:, None]).reshape(experts, pairs)
    hits = (expert_ids.reshape(experts, pairs) == index).astype(jnp.int32)
    ranks = jnp.cumsum(hits, axis=1, dtype=jnp.int32)
    levels = jnp.arange(1, capacity + 1, dtype=jnp.int32)
    select = hits[:, None, :] * (ranks[:, None, :] == levels[None, :, None]).astype(jnp.int32)
    pair_row = jnp.arange(pairs, dtype=jnp.int32) // TOPK
    local_row = lax.optimization_barrier(jnp.sum(select * pair_row[None, None, :], axis=-1, dtype=jnp.int32))
    filled = lax.optimization_barrier(jnp.sum(select, axis=-1, dtype=jnp.int32)).reshape(-1)
    slot_weight = lax.optimization_barrier(jnp.sum(select.astype(jnp.float32) * pair_weight[:, None, :], axis=-1)).reshape(-1)
    row_index = (local_row + jnp.arange(experts, dtype=jnp.int32)[:, None] * rows_each).reshape(-1)
    return (row_index, filled, slot_weight)

def reference(resid, proj_x, proj_z, proj_bc, proj_dt, tail_x, tail_bc, taps_x, taps_bc, ssm_state, dt_bias, decay_log, group_gain, out_proj, ffn_gain, dense_gate, dense_up, dense_down, branch_gate, group_weights, expert_ids, expert_weights, exp_gate, exp_up, exp_down):
    y_out, new_state = state_update(proj_x, proj_z, proj_bc, proj_dt, tail_x, tail_bc, taps_x, taps_bc, ssm_state, dt_bias, decay_log, group_gain)
    mixed = jnp.dot(y_out, out_proj, preferred_element_type=jnp.float32)
    resid_new = (resid.astype(jnp.float32) + mixed).astype(jnp.bfloat16)
    widened = resid_new.astype(jnp.float32)
    normed = (widened * lax.rsqrt(lax.optimization_barrier(jnp.mean(widened * widened, axis=-1, keepdims=True)) + EPSILON) * ffn_gain).astype(jnp.bfloat16)
    score = jnp.dot(normed, branch_gate, preferred_element_type=jnp.float32)
    dense_pre = jnp.dot(normed, dense_gate, preferred_element_type=jnp.float32)
    dense_lin = jnp.dot(normed, dense_up, preferred_element_type=jnp.float32)
    dense_hidden = (jax.nn.sigmoid(score)[:, None] * jax.nn.silu(dense_pre) * dense_lin).astype(jnp.bfloat16)
    total = jnp.dot(dense_hidden, dense_down, preferred_element_type=jnp.float32)

    def expert_step(accum, items):
        gate_w, up_w, down_w, index = items
        row_index, filled, slot_weight = expert_slots(expert_ids, expert_weights, group_weights, index, EXPERTS, EPG, CAP)
        slot_rows = jnp.take(normed, row_index, axis=0)
        slot_pre = jnp.dot(slot_rows, gate_w, preferred_element_type=jnp.float32)
        slot_lin = jnp.dot(slot_rows, up_w, preferred_element_type=jnp.float32)
        slot_hidden = (slot_weight[:, None] * jax.nn.silu(slot_pre) * slot_lin).astype(jnp.bfloat16)
        slot_out = jnp.dot(slot_hidden, down_w, preferred_element_type=jnp.float32)
        slot_out = slot_out * (filled > 0).astype(jnp.float32)[:, None]
        return (accum.at[row_index].add(slot_out), None)
    total, _ = lax.scan(expert_step, total, (exp_gate, exp_up, exp_down, jnp.arange(EXPERTS, dtype=jnp.int32)))
    out = (widened + total).astype(jnp.bfloat16)
    return (out, new_state)
```

```python
import functools

import jax
import jax.numpy as jnp
from jax import lax
from jax.experimental import pallas as pl
from jax.experimental.pallas import tpu as pltpu
from jax.sharding import Mesh
from jax.sharding import PartitionSpec as P

F32, BF16, I32 = jnp.float32, jnp.bfloat16, jnp.int32
EP = ("z", "y", "x")
EP_TP = ("z", "y", "x", "tp")
NZ, NY, NX = 8, 4, 4
EPSILON = 1e-06
MESH = pl.DeviceIdType.MESH
VMEM = pltpu.MemorySpace.VMEM
CHUNKS = 8


def dot(a, b):
    return lax.dot_general(a, b, (((1,), (0,)), ((), ())), preferred_element_type=F32)


def dot_t(a, b):
    return lax.dot_general(a, b, (((1,), (1,)), ((), ())), preferred_element_type=F32)


def silu(v):
    return v / (1.0 + jnp.exp(-v))


def iota(shape, dim):
    return lax.broadcasted_iota(I32, shape, dim)


def split(v):
    high = v.astype(BF16)
    return high, (v - high.astype(F32)).astype(BF16)


def spread(v, width):
    total = v.shape[1]
    heads = total // width
    per = 16 // heads
    mask = (iota((16, total), 1) // width) == (iota((16, total), 0) // per)
    rows = jnp.where(mask[None], jnp.broadcast_to(v[:, None, :], (16, 16, total)), 0.0).reshape(256, total)
    pick = ((iota((total, 128), 0) % width) == (iota((total, 128), 1) % width)).astype(BF16)
    high, low = split(rows)
    return dot(high, pick) + dot(low, pick)


def local_kernel(px, pz, bc, pdt, tx, wx, dtb, dlg, gg, ids, ew, gw, state, new_state, y_out, disp, c_hi, c_lo,
                 sbuf, route, xs_s, in_s, rd_s, de_s, rdo, isem, osem):
    def in_copy(j):
        return pltpu.make_async_copy(state.at[:, :, pl.ds(pl.multiple_of(j * 512, 512), 512)], sbuf.at[j], isem.at[j])

    def out_copy(j):
        return pltpu.make_async_copy(sbuf.at[j], new_state.at[:, :, pl.ds(pl.multiple_of(j * 512, 512), 512)], osem.at[j])

    for j in range(CHUNKS):
        in_copy(j).start()
    conv_x = px[...].astype(F32) * wx[3:4, :].astype(F32)
    for w in range(3):
        conv_x = conv_x + tx[w].astype(F32) * wx[w : w + 1, :].astype(F32)
    conv_x = silu(conv_x)
    pre = pdt[...].astype(F32) + dtb[...]
    step = jnp.maximum(pre, 0.0) + jnp.log1p(jnp.exp(-jnp.abs(pre)))
    decay = jnp.exp(-step * jnp.exp(dlg[...]))
    eye = (iota((16, 16), 0) == iota((16, 16), 1))[None]

    def column(v):
        wide = jnp.where(eye, jnp.broadcast_to(v[:, None, :], (16, 16, 16)), 0.0)
        return jnp.sum(wide, axis=-1, keepdims=True).reshape(256, 1)

    x_rows = spread(conv_x, 64) * column(step)
    high, low = split(x_rows)
    xs_s[...] = jnp.where(iota((256, 128), 1) < 64, high.astype(F32), low.astype(F32)).astype(BF16)
    in_s[...] = spread(bc[0], 64)
    rd_s[...] = spread(bc[1], 64)
    de_s[...] = jnp.broadcast_to(column(decay), (256, 128))
    rdo[...] = jnp.zeros_like(rdo)

    def chunk(j, carry):
        in_copy(j).wait()
        grid = ((iota((128, 512), 0) % 64) == (iota((128, 512), 1) // 64 + j * 8)).astype(BF16)
        fresh = dot(xs_s[...], grid)
        old = sbuf[j].reshape(256, 512)
        new = jnp.tile(de_s[...], (1, 4)) * old + fresh * jnp.tile(in_s[...], (1, 4))
        sbuf[j] = new.reshape(16, 16, 512)
        rdo[...] += dot_t((new * jnp.tile(rd_s[...], (1, 4))).astype(BF16), grid)
        return carry

    def chunk_out(j, carry):
        chunk(j, carry)
        out_copy(j).start()
        return carry

    lax.fori_loop(0, CHUNKS, chunk_out, 0)

    wide = jnp.tile(rdo[...], (1, 8))
    keep = (iota((16, 1024), 1) // 64) == iota((16, 1024), 0)
    read = jnp.sum(jnp.where(keep[None], wide.reshape(16, 16, 1024), 0.0), axis=1)
    gated = read * silu(pz[...].astype(F32))
    for g in range(4):
        part = gated[:, g * 256 : (g + 1) * 256]
        scale = lax.rsqrt(jnp.mean(part * part, axis=-1, keepdims=True) + EPSILON)
        y_out[:, g * 256 : (g + 1) * 256] = (part * scale * gg[:, g * 256 : (g + 1) * 256]).astype(BF16)

    z, q = lax.axis_index("z"), lax.axis_index("y") * NX + lax.axis_index("x")
    route[...] = jnp.zeros_like(route)
    route[0:6, :] = ids[...].astype(F32)
    route[8:14, :] = ew[...]
    route[16:20, :] = gw[...]
    row, tok = iota((2048, 128), 0), iota((2048, 128), 1)
    take = (row == (tok // 16) * 256 + q * 16 + tok % 16).astype(BF16)
    high, rest = split(route[...])
    mine = dot(high, take) + dot(rest, take)
    own = iota((16, 128), 0) + z * 16
    hit = jnp.zeros((16, 128), F32)
    weight = jnp.zeros((16, 128), F32)
    for k in range(6):
        same = mine[k : k + 1, :].astype(I32) == own
        hit = hit + same.astype(F32)
        weight = weight + jnp.where(same, mine[8 + k : 9 + k, :], 0.0)
    coarse = jnp.sum(jnp.where(iota((8, 128), 0) == z // 2, mine[16:24, :], 0.0), axis=0, keepdims=True)
    weight = weight * coarse
    a, b = iota((128, 128), 0), iota((128, 128), 1)
    before = ((a // 16 == b // 16) & (a < b)).astype(BF16)
    rank = dot(hit.astype(BF16), before)
    slot, tok3 = iota((16, 16, 128), 1), iota((16, 16, 128), 2)
    chosen = (
        (hit[:, None, :] > 0.5)
        & (rank[:, None, :] == (slot % 2).astype(F32))
        & (slot // 2 == tok3 // 16)
    )
    disp[...] = jnp.where(chosen, 1.0, 0.0).reshape(256, 128).astype(BF16)
    comb = jnp.where(chosen, jnp.broadcast_to(weight[:, None, :], (16, 16, 128)), 0.0).reshape(256, 128)
    comb = jnp.concatenate([comb[:128].T, comb[128:].T], axis=1)
    high, low = split(comb)
    c_hi[...] = high
    c_lo[...] = low
    for j in range(CHUNKS):
        out_copy(j).wait()


class Copies:
    def __init__(self, sems):
        self.sems, self.started = sems, []

    def __call__(self, src, dst, recv, **where):
        copy = pltpu.make_async_remote_copy(
            src_ref=src, dst_ref=dst, send_sem=self.sems.at[len(self.started)], recv_sem=recv,
            device_id=where, device_id_type=MESH,
        )
        copy.start()
        self.started.append(copy)

    def arrived(self, ref, recv, **where):
        pltpu.make_async_remote_copy(
            src_ref=ref, dst_ref=ref, send_sem=self.sems.at[0], recv_sem=recv, device_id=where, device_id_type=MESH,
        ).wait_recv()

    def drain(self):
        for copy in self.started:
            copy.wait_send()


def plane_gather(copies, buf, lane, width, g, rsem, coords):
    fa, sa = ("x", "y") if g == 0 else ("y", "x")
    f, s = coords[fa], coords[sa]

    def place(df, ds):
        fv, sv = lax.rem(f + df + 4, 4), lax.rem(s + ds + 4, 4)
        return sv * 4 + fv if g == 0 else fv * 4 + sv

    def piece(qi, part):
        start, size = (lane, width) if part == 0 else (lane + (part - 1) * (width // 2), width // 2)
        lead = (qi,) + (slice(None),) * (len(buf.shape) - 2)
        return buf.at[lead + (pl.ds(start, size),)]

    def send(df, ds, part, axis, move):
        qi = place(df, ds)
        ref = piece(qi, part)
        copies(ref, ref, rsem.at[g, qi, 1 if part == 2 else 0], **{axis: lax.rem(coords[axis] + move + 4, 4)})

    def wait(df, ds, part):
        qi = place(df, ds)
        copies.arrived(piece(qi, part), rsem.at[g, qi, 1 if part == 2 else 0], **{fa: lax.rem(f + 1, 4)})

    for move in (1, -1):
        send(0, 0, 0, fa, move)
    for move in (1, -1):
        send(0, 0, 0, sa, move)
    yield
    for df, part in ((-1, 1), (1, 2)):
        wait(df, 0, 0)
        send(df, 0, part, fa, -df)
        for move in (1, -1):
            send(df, 0, 0, sa, move)
    yield
    wait(2, 0, 1)
    wait(2, 0, 2)
    for move in (1, -1):
        send(2, 0, 0, sa, move)
    yield
    for df in (0, -1, 1, 2):
        for ds, part in ((-1, 1), (1, 2)):
            wait(df, ds, 0)
            send(df, ds, part, sa, -ds)
    yield
    for df in (0, -1, 1, 2):
        wait(df, 2, 1)
        wait(df, 2, 2)
    yield


Z_ORDER = (4, 3, 5, 2, 6, 1, 7)
PLANE_ORDER = ((2, 2), (1, 2), (3, 2), (2, 1), (2, 3), (2, 0), (0, 2), (1, 1), (1, 3), (3, 1), (3, 3), (1, 0), (3, 0), (0, 1), (0, 3))


def mesh_kernel(y_ref, r_ref, ot_ref, gt_ref, ut_ref, dn_ref, gain, bgate, disp, c_hi, c_lo, eg_hbm, eu_hbm, ed_hbm, out_ref,
                wbuf, obuf, ybuf, rbuf, mown, msend, mrecv, nbuf, rn, normed, dsend, drecv, xsend, xfull, esend, erecv,
                csend, cbuf, tot, zsend, zrecv, fin, frecv, eg, eu, ed,
                ssem, wsem, gsem, zsem, asem, tsem, nsem, fsem, lsem):
    z, y, x, t = (lax.axis_index(a) for a in EP_TP)
    coords = {"x": x, "y": y}
    q = y * 4 + x
    other = 1 - t
    planes = [(lax.rem(y + dy, 4), lax.rem(x + dx, 4)) for dy, dx in PLANE_ORDER]
    zs = [lax.rem(z + d, 8) for d in Z_ORDER]

    loads = [pltpu.make_async_copy(src.at[0], dst, lsem.at[i]) for i, (src, dst) in enumerate(((eg_hbm, eg), (eu_hbm, eu), (ed_hbm, ed)))]
    for load in loads:
        load.start()

    barrier = pltpu.get_barrier_semaphore()
    for zz in zs:
        pl.semaphore_signal(barrier, inc=1, device_id={"z": zz}, device_id_type=MESH)
    for yy, xx in planes:
        pl.semaphore_signal(barrier, inc=1, device_id={"y": yy, "x": xx}, device_id_type=MESH)
    pl.semaphore_signal(barrier, inc=1, device_id={"tp": other}, device_id_type=MESH)
    obuf[q] = ot_ref[...]
    wbuf[q, 0] = gt_ref[...]
    wbuf[q, 1] = ut_ref[...]
    wbuf[q, 2] = dn_ref[...]
    ybuf[z] = y_ref[...]
    pl.semaphore_wait(barrier, len(zs) + len(planes) + 1)

    copies = Copies(ssem)
    for zz in zs:
        copies(y_ref, ybuf.at[z], zsem.at[0, z], z=zz)
    for zz in zs:
        copies(r_ref.at[:, pl.ds(pl.multiple_of(zz * 256 + t * 128, 128), 128)], rbuf.at[z], zsem.at[1, z], z=zz)
    og = [plane_gather(copies, obuf, g * 512, 512, g, gsem, coords) for g in range(2)]
    wg = [plane_gather(copies, wbuf, g * 1024, 1024, g, wsem, coords) for g in range(2)]

    def advance(gens):
        for gen in gens:
            next(gen)

    advance(og)
    advance(wg)
    rbuf[z] = r_ref[:, pl.ds(pl.multiple_of(z * 256 + t * 128, 128), 128)]
    advance(og)
    advance(og)
    advance(wg)
    advance(og)
    advance(og)
    for zz in zs:
        copies.arrived(ybuf.at[zz], zsem.at[0, zz], z=zz)

    rows = ybuf[...].reshape(128, 1024)
    mown[...] = dot_t(rows, obuf[pl.ds(t * 8, 8)].reshape(128, 1024))
    msend[...] = dot_t(rows, obuf[pl.ds(other * 8, 8)].reshape(128, 1024)).astype(BF16)
    copies(msend, mrecv, tsem.at[0], tp=other)
    advance(wg)
    for zz in zs:
        copies.arrived(rbuf.at[zz], zsem.at[1, zz], z=zz)
    copies.arrived(mrecv, tsem.at[0], tp=other)
    mixed = mown[...] + mrecv[...].astype(F32)
    nbuf[z, t] = (rbuf[...].reshape(128, 128).astype(F32) + mixed).astype(BF16)
    for zz in zs:
        copies(nbuf.at[z, t], nbuf.at[z, t], zsem.at[2, z], z=zz)
    copies(nbuf.at[z, t], nbuf.at[z, t], nsem.at[z], tp=other)
    advance(wg)
    for zz in zs[::-1]:
        copies.arrived(nbuf.at[zz, t], zsem.at[2, zz], z=zz)
        copies(nbuf.at[zz, t], nbuf.at[zz, t], nsem.at[zz], tp=other)
    for zz in zs[::-1] + [z]:
        copies.arrived(nbuf.at[zz, other], nsem.at[zz], tp=other)

    for j in range(16):
        rn[:, j * 128 : (j + 1) * 128] = nbuf[j // 2, j % 2]
    wide = rn[...].astype(F32)
    scale = lax.rsqrt(jnp.mean(wide * wide, axis=-1, keepdims=True) + EPSILON)
    normed[...] = (wide * scale * gain[...]).astype(BF16)
    half = pl.ds(pl.multiple_of(t * 1024, 1024), 1024)
    far = pl.ds(pl.multiple_of(other * 1024, 1024), 1024)

    xsend[...] = dot(disp[...], normed[:, half]).astype(BF16).reshape(16, 16, 1024)
    for yy, xx in planes:
        copies(xsend.at[yy * 4 + xx], xfull.at[t, q], asem.at[0, q], y=yy, x=xx)
    xfull[t, q] = xsend[q]
    copies(xsend.at[q], xfull.at[t, q], fsem.at[q], tp=other)

    advance(wg)
    tokens = normed[...]
    score = jnp.sum(tokens.astype(F32) * bgate[...].astype(F32), axis=-1, keepdims=True)
    gate = dot_t(tokens, wbuf[:, 0].reshape(256, 2048))
    lin = dot_t(tokens, wbuf[:, 1].reshape(256, 2048))
    hidden = (silu(gate) * lin / (1.0 + jnp.exp(-score))).astype(BF16)
    dsend[...] = dot(hidden, wbuf[:, 2, :, far].reshape(256, 1024)).astype(BF16)
    copies(dsend, drecv, tsem.at[1], tp=other)
    tot[...] = dot(hidden, wbuf[:, 2, :, half].reshape(256, 1024)).reshape(8, 16, 1024)

    for yy, xx in planes[::-1]:
        qq = yy * 4 + xx
        copies.arrived(xfull.at[t, qq], asem.at[0, qq], y=yy, x=xx)
        copies(xfull.at[t, qq], xfull.at[t, qq], fsem.at[qq], tp=other)
    for yy, xx in planes[::-1] + [(y, x)]:
        qq = yy * 4 + xx
        copies.arrived(xfull.at[other, qq], fsem.at[qq], tp=other)
    for load in loads:
        load.wait()
    left, right = xfull[0].reshape(256, 1024), xfull[1].reshape(256, 1024)
    gate = dot(left, eg[0:1024, :]) + dot(right, eg[1024:2048, :])
    lin = dot(left, eu[0:1024, :]) + dot(right, eu[1024:2048, :])
    hidden = (silu(gate) * lin).astype(BF16)
    esend[...] = dot(hidden, ed[:, far]).astype(BF16)
    copies(esend, erecv, tsem.at[2], tp=other)
    mine = dot(hidden, ed[:, half])
    copies.arrived(erecv, tsem.at[2], tp=other)
    csend[...] = (mine + erecv[...].astype(F32)).astype(BF16).reshape(16, 16, 1024)
    for yy, xx in planes:
        copies(csend.at[yy * 4 + xx], cbuf.at[q], asem.at[1, q], y=yy, x=xx)
    cbuf[q] = csend[q]
    copies.arrived(drecv, tsem.at[1], tp=other)
    tot[...] = tot[...] + drecv[...].astype(F32).reshape(8, 16, 1024)
    for yy, xx in planes[::-1]:
        qq = yy * 4 + xx
        copies.arrived(cbuf.at[qq], asem.at[1, qq], y=yy, x=xx)
    back = cbuf[...].reshape(256, 1024)
    total = tot[...].reshape(128, 1024) + dot(c_hi[...], back) + dot(c_lo[...], back)
    tot[...] = total.reshape(8, 16, 1024)
    zsend[...] = total.astype(BF16).reshape(8, 16, 1024)
    for zz in zs:
        copies(zsend.at[zz], zrecv.at[z], zsem.at[3, z], z=zz)
    final = tot[z] + rn[pl.ds(pl.multiple_of(z * 16, 16), 16), half].astype(F32)
    for zz in zs[::-1]:
        copies.arrived(zrecv.at[zz], zsem.at[3, zz], z=zz)
        final = final + zrecv[zz].astype(F32)
    fin[...] = final
    copies(fin.at[pl.ds(pl.multiple_of(other * 8, 8), 8)], frecv, tsem.at[3], tp=other)
    out_ref[:, half] = fin[pl.ds(pl.multiple_of(t * 8, 8), 8), :].astype(BF16)
    copies.arrived(frecv, tsem.at[3], tp=other)
    out_ref[:, far] = frecv[...].astype(BF16)
    copies.drain()


def shards(resid, proj_x, proj_z, proj_bc, proj_dt, tail_x, tail_bc, taps_x, taps_bc, ssm_state, dt_bias, decay_log,
           group_gain, out_proj, ffn_gain, dense_gate, dense_up, dense_down, branch_gate, group_weights, expert_ids,
           expert_weights, exp_gate, exp_up, exp_down):
    window = jnp.concatenate([tail_bc, proj_bc[:, None]], axis=1).astype(F32)
    bc = jax.nn.silu(jnp.sum(window * taps_bc.astype(F32)[None], axis=1)).transpose(1, 0, 2)
    vm = pl.BlockSpec(memory_space=VMEM)
    hbm = pl.BlockSpec(memory_space=pl.ANY)
    new_state, y_out, disp, c_hi, c_lo = pl.pallas_call(
        local_kernel,
        out_shape=(
            jax.ShapeDtypeStruct((16, 16, 4096), F32),
            jax.ShapeDtypeStruct((16, 1024), BF16),
            jax.ShapeDtypeStruct((256, 128), BF16),
            jax.ShapeDtypeStruct((128, 256), BF16),
            jax.ShapeDtypeStruct((128, 256), BF16),
        ),
        in_specs=[vm] * 12 + [hbm],
        out_specs=(hbm, vm, vm, vm, vm),
        scratch_shapes=[
            pltpu.VMEM((CHUNKS, 16, 16, 512), F32),
            pltpu.VMEM((32, 2048), F32),
            pltpu.VMEM((256, 128), BF16),
            pltpu.VMEM((256, 128), F32),
            pltpu.VMEM((256, 128), F32),
            pltpu.VMEM((256, 128), F32),
            pltpu.VMEM((256, 128), F32),
            pltpu.SemaphoreType.DMA((CHUNKS,)),
            pltpu.SemaphoreType.DMA((CHUNKS,)),
        ],
        compiler_params=pltpu.CompilerParams(vmem_limit_bytes=32 << 20),
        name="state",
    )(proj_x, proj_z, bc, proj_dt, tail_x.transpose(1, 0, 2), taps_x, dt_bias.reshape(1, 16), decay_log.reshape(1, 16),
      group_gain.reshape(1, 1024), expert_ids.T, expert_weights.T, group_weights.T, ssm_state)
    out = pl.pallas_call(
        mesh_kernel,
        out_shape=jax.ShapeDtypeStruct((8, 2048), BF16),
        in_specs=[vm] * 11 + [hbm] * 3,
        out_specs=vm,
        scratch_shapes=[
            pltpu.VMEM((16, 3, 16, 2048), BF16),
            pltpu.VMEM((16, 16, 1024), BF16),
            pltpu.VMEM((8, 16, 1024), BF16),
            pltpu.VMEM((8, 16, 128), BF16),
            pltpu.VMEM((128, 128), F32),
            pltpu.VMEM((128, 128), BF16),
            pltpu.VMEM((128, 128), BF16),
            pltpu.VMEM((8, 2, 128, 128), BF16),
            pltpu.VMEM((128, 2048), BF16),
            pltpu.VMEM((128, 2048), BF16),
            pltpu.VMEM((128, 1024), BF16),
            pltpu.VMEM((128, 1024), BF16),
            pltpu.VMEM((16, 16, 1024), BF16),
            pltpu.VMEM((2, 16, 16, 1024), BF16),
            pltpu.VMEM((256, 1024), BF16),
            pltpu.VMEM((256, 1024), BF16),
            pltpu.VMEM((16, 16, 1024), BF16),
            pltpu.VMEM((16, 16, 1024), BF16),
            pltpu.VMEM((8, 16, 1024), F32),
            pltpu.VMEM((8, 16, 1024), BF16),
            pltpu.VMEM((8, 16, 1024), BF16),
            pltpu.VMEM((16, 1024), F32),
            pltpu.VMEM((8, 1024), F32),
            pltpu.VMEM((2048, 256), BF16),
            pltpu.VMEM((2048, 256), BF16),
            pltpu.VMEM((256, 2048), BF16),
            pltpu.SemaphoreType.DMA((192,)),
            pltpu.SemaphoreType.DMA((2, 16, 2)),
            pltpu.SemaphoreType.DMA((2, 16, 2)),
            pltpu.SemaphoreType.DMA((4, 8)),
            pltpu.SemaphoreType.DMA((2, 16)),
            pltpu.SemaphoreType.DMA((4,)),
            pltpu.SemaphoreType.DMA((8,)),
            pltpu.SemaphoreType.DMA((16,)),
            pltpu.SemaphoreType.DMA((3,)),
        ],
        compiler_params=pltpu.CompilerParams(collective_id=0, has_side_effects=True, vmem_limit_bytes=48 << 20),
        name="mesh",
    )(y_out, resid, out_proj.T, dense_gate.T, dense_up.T, dense_down, ffn_gain.reshape(1, 2048),
      branch_gate.reshape(1, 2048), disp, c_hi, c_lo, exp_gate, exp_up, exp_down)
    return (out, new_state)


def solution(mesh):
    finer = Mesh(mesh.devices.reshape(NZ, NY, NX, mesh.shape["tp"]), EP_TP)
    in_specs = (
        P(EP, None), P(EP, "tp"), P(EP, "tp"), P(EP, None, "tp"), P(EP, "tp"), P(EP, None, "tp"), P(EP, None, None, "tp"),
        P(None, "tp"), P(None, None, "tp"), P(EP, "tp", None), P("tp"), P("tp"), P("tp"), P("tp", EP), P(),
        P(None, EP_TP), P(None, EP_TP), P(EP_TP, None), P(), P(), P(), P(), P(EP, None, "tp"), P(EP, None, "tp"),
        P(EP, "tp", None),
    )
    out_specs = (P(EP_TP, None), P(EP, "tp", None))
    return jax.shard_map(shards, mesh=finer, in_specs=in_specs, out_specs=out_specs, check_vma=False)
```

```python
import functools

import jax
import jax.numpy as jnp
from jax import lax
from jax.experimental import pallas as pl
from jax.experimental.pallas import tpu as pltpu
from jax.sharding import Mesh
from jax.sharding import PartitionSpec as P

F32, BF16, I32 = jnp.float32, jnp.bfloat16, jnp.int32
EP = ("z", "y", "x")
EP_TP = ("z", "y", "x", "tp")
NZ, NY, NX = 8, 4, 4
EPSILON = 1e-06
MESH = pl.DeviceIdType.MESH
VMEM = pltpu.MemorySpace.VMEM
CHUNKS = 4
WIDE = 4096 // CHUNKS
EARLY = 11
SMALL = 14


def dot(a, b):
    return lax.dot_general(a, b, (((1,), (0,)), ((), ())), preferred_element_type=F32)


def dot_t(a, b):
    return lax.dot_general(a, b, (((1,), (1,)), ((), ())), preferred_element_type=F32)


def silu(v):
    return v / (1.0 + jnp.exp(-v))


def iota(shape, dim):
    return lax.broadcasted_iota(I32, shape, dim)


def split(v):
    high = v.astype(BF16)
    return high, (v - high.astype(F32)).astype(BF16)


def spread(v):
    total = v.shape[1]
    per = 8 // (total // 64)
    mask = (iota((8, total), 1) // 64) == (iota((8, total), 0) // per)
    rows = jnp.where(mask[None], jnp.broadcast_to(v[:, None, :], (16, 8, total)), 0.0).reshape(128, total)
    pick = ((iota((total, 128), 0) % 64) == (iota((total, 128), 1) % 64)).astype(BF16)
    high, low = split(rows)
    return dot(high, pick) + dot(low, pick)


def column(v, half):
    mine = (iota((8, 16), 1) == iota((8, 16), 0) + half * 8)[None]
    wide = jnp.where(mine, jnp.broadcast_to(v[:, None, :], (16, 8, 16)), 0.0)
    return jnp.sum(wide, axis=-1, keepdims=True).reshape(128, 1)


class Copies:
    def __init__(self, sems):
        self.sems, self.started = sems, []

    def __call__(self, src, dst, recv, **where):
        copy = pltpu.make_async_remote_copy(
            src_ref=src, dst_ref=dst, send_sem=self.sems.at[len(self.started)], recv_sem=recv,
            device_id=where, device_id_type=MESH,
        )
        copy.start()
        self.started.append(copy)

    def arrived(self, ref, recv, **where):
        pltpu.make_async_remote_copy(
            src_ref=ref, dst_ref=ref, send_sem=self.sems.at[0], recv_sem=recv, device_id=where, device_id_type=MESH,
        ).wait_recv()

    def drain(self):
        for copy in self.started:
            copy.wait_send()


def plane_gather(copies, buf, lane, width, g, rsem, coords):
    fa, sa = ("x", "y") if g == 0 else ("y", "x")
    f, s = coords[fa], coords[sa]

    def place(df, ds):
        fv, sv = lax.rem(f + df + 4, 4), lax.rem(s + ds + 4, 4)
        return sv * 4 + fv if g == 0 else fv * 4 + sv

    def piece(qi, part):
        start, size = (lane, width) if part == 0 else (lane + (part - 1) * (width // 2), width // 2)
        lead = (qi,) + (slice(None),) * (len(buf.shape) - 2)
        return buf.at[lead + (pl.ds(start, size),)]

    def send(df, ds, part, axis, move):
        qi = place(df, ds)
        ref = piece(qi, part)
        copies(ref, ref, rsem.at[g, qi, 1 if part == 2 else 0], **{axis: lax.rem(coords[axis] + move + 4, 4)})

    def wait(df, ds, part):
        qi = place(df, ds)
        copies.arrived(piece(qi, part), rsem.at[g, qi, 1 if part == 2 else 0], **{fa: lax.rem(f + 1, 4)})

    turns = ((-1, 1), (1, 2))
    for axis in (fa, sa):
        for move in (1, -1):
            send(0, 0, 0, axis, move)
    yield
    for df, part in turns:
        wait(df, 0, 0)
        send(df, 0, part, fa, -df)
    for ds, part in turns:
        wait(0, ds, 0)
        send(0, ds, part, sa, -ds)
    yield
    for df in (-1, 1):
        for move in (1, -1):
            send(df, 0, 0, sa, move)
    yield
    wait(2, 0, 1)
    wait(2, 0, 2)
    for move in (1, -1):
        send(2, 0, 0, sa, move)
    for df in (-1, 1):
        for ds, part in turns:
            wait(df, ds, 0)
            send(df, ds, part, sa, -ds)
    yield
    for ds, part in turns:
        wait(2, ds, 0)
        send(2, ds, part, sa, -ds)
    yield
    for df in (0, -1, 1, 2):
        wait(df, 2, 1)
        wait(df, 2, 2)
    yield


Z_ORDER = (4, 3, 5, 2, 6, 1, 7)
SENDS = ((2, 2), (2, 1), (2, 3), (2, 0), (1, 2), (1, 1), (1, 3), (1, 0), (3, 2), (3, 1), (3, 3), (3, 0), (0, 2), (0, 1), (0, 3))
WAVES = (2, 3, 1, 0)


def mesh_kernel(*refs):
    small, (state, r_hbm, ot_hbm, gt_hbm, ut_hbm, dn_hbm, gain_hbm, bg_hbm, eg_hbm, eu_hbm, ed_hbm) = refs[:SMALL], refs[SMALL : SMALL + 11]
    new_state, out_ref = refs[SMALL + 11 : SMALL + 13]
    refs = refs[SMALL + 13 :]
    px, pz, pb, pdt, tx, tb, wx, wb, dtb, dlg, gg, ids, ew, gw = refs[:SMALL]
    (route, grid, xs_s, in_s, rd_s, de_s, rdo, disp, c_hi, c_lo, r_ref, gain, bgate,
     wbuf, obuf, ybuf, rbuf, mown, msend, mrecv, nbuf, rn, normed, dsend, drecv, xsend, xfull, emine, esend, erecv,
     csend, cbuf, tot, zsend, zrecv, fin, eg, eu, ed,
     ssem, wsem, gsem, zsem, asem, tsem, nsem, fsem, rsem, lsem, msem, isem) = refs[SMALL:]
    z, y, x, t = (lax.axis_index(a) for a in EP_TP)
    coords = {"x": x, "y": y}
    q = y * 4 + x
    other = 1 - t
    sends = [(lax.rem(y + dy, 4), lax.rem(x + dx, 4)) for dy, dx in SENDS]
    waves = [[(lax.rem(y + dy, 4), lax.rem(x + dx, 4), dy == 0 and dx == 0) for dx in (2, 3, 1, 0)] for dy in WAVES]
    zs = [lax.rem(z + d, 8) for d in Z_ORDER]

    barrier = pltpu.get_barrier_semaphore()
    for zz in zs:
        pl.semaphore_signal(barrier, inc=1, device_id={"z": zz}, device_id_type=MESH)
    for yy, xx in sends:
        pl.semaphore_signal(barrier, inc=1, device_id={"y": yy, "x": xx}, device_id_type=MESH)
    pl.semaphore_signal(barrier, inc=1, device_id={"tp": other}, device_id_type=MESH)
    for zz in zs:
        pl.semaphore_signal(barrier, inc=1, device_id={"z": zz, "tp": other}, device_id_type=MESH)

    def block(ref, half, j):
        return ref.at[:, pl.ds(half * 8, 8), pl.ds(j * WIDE, WIDE)]

    def in_copy(half, j):
        return pltpu.make_async_copy(block(state, half, j), block(new_state, half, j), isem.at[half, j])

    first = [pltpu.make_async_copy(src, dst, msem.at[i]) for i, (src, dst) in enumerate(zip(small, refs[:SMALL]))]
    for load in first[:EARLY]:
        load.start()
    for half in range(2):
        for j in range(CHUNKS):
            in_copy(half, j).start()
    pairs = ((ot_hbm, obuf.at[q]), (gt_hbm, wbuf.at[q, 0]), (ut_hbm, wbuf.at[q, 1]), (dn_hbm, wbuf.at[q, 2]), (r_hbm, r_ref),
             (gain_hbm, gain), (bg_hbm, bgate), (eg_hbm.at[0], eg), (eu_hbm.at[0], eu), (ed_hbm.at[0], ed))
    loads = [pltpu.make_async_copy(src, dst, lsem.at[i]) for i, (src, dst) in enumerate(pairs)]
    grid[...] = ((iota((128, WIDE), 0) % 64) == (iota((128, WIDE), 1) // 64)).astype(BF16)
    for load in first[:EARLY]:
        load.wait()
    for load in first[EARLY:] + loads[:5]:
        load.start()

    conv_x = px[...].astype(F32) * wx[3:4, :].astype(F32)
    for w in range(3):
        conv_x = conv_x + tx[w].astype(F32) * wx[w : w + 1, :].astype(F32)
    conv_x = silu(conv_x)
    conv_bc = pb[...].astype(F32) * wb[3:4].astype(F32)
    for w in range(3):
        conv_bc = conv_bc + tb[:, w].astype(F32) * wb[w : w + 1].astype(F32)
    conv_bc = silu(conv_bc)
    top = iota((16, 2, 256), 1) == 0
    inputs = jnp.sum(jnp.where(top, conv_bc, 0.0), axis=1)
    reads = jnp.sum(jnp.where(top, 0.0, conv_bc), axis=1)
    pre = pdt[...].astype(F32) + dtb[...]
    step = jnp.maximum(pre, 0.0) + jnp.log1p(jnp.exp(-jnp.abs(pre)))
    decay = jnp.exp(-step * jnp.exp(dlg[...]))
    for half in range(2):
        x_rows = spread(conv_x[:, half * 512 : (half + 1) * 512]) * column(step, half)
        high, low = split(x_rows)
        xs_s[half] = jnp.where(iota((128, 128), 1) < 64, high.astype(F32), low.astype(F32))
        in_s[half] = spread(inputs[:, half * 128 : (half + 1) * 128])
        rd_s[half] = spread(reads[:, half * 128 : (half + 1) * 128])
        de_s[half] = jnp.broadcast_to(column(decay, half), (128, 128))

    def advance_state(half, low, high):
        lanes = WIDE // 64
        for j in range(low, high):
            in_copy(half, j).wait()
            here = (slice(None), slice(half * 8, half * 8 + 8), slice(j * WIDE, (j + 1) * WIDE))
            shifted = xs_s[half] if j == 0 else pltpu.roll(xs_s[half], 128 - j * lanes, 1)
            fresh = dot(shifted.astype(BF16), grid[...])
            new = jnp.tile(de_s[half], (1, WIDE // 128)) * new_state[here].reshape(128, WIDE) + fresh * jnp.tile(in_s[half], (1, WIDE // 128))
            new_state[here] = new.reshape(16, 8, WIDE)
            part = dot_t((new * jnp.tile(rd_s[half], (1, WIDE // 128))).astype(BF16), grid[...])
            rdo[half] = part if j == 0 else rdo[half] + pltpu.roll(part, j * lanes, 1)

    def finish_state(half):
        keep = (iota((8, 512), 1) // 64) == iota((8, 512), 0)
        wide = jnp.tile(rdo[half], (1, 4)).reshape(16, 8, 512)
        read = jnp.sum(jnp.where(keep[None], wide, 0.0), axis=1)
        gated = read * silu(pz[:, half * 512 : (half + 1) * 512].astype(F32))
        for g in range(2):
            lanes = slice(half * 512 + g * 256, half * 512 + (g + 1) * 256)
            part = gated[:, g * 256 : (g + 1) * 256]
            scale = lax.rsqrt(jnp.mean(part * part, axis=-1, keepdims=True) + EPSILON)
            ybuf[z, :, lanes] = (part * scale * gg[:, lanes]).astype(BF16)

    copies = Copies(ssem)

    def send_y(half):
        ref = ybuf.at[z, :, half * 512 : (half + 1) * 512]
        for zz in zs:
            copies(ref, ref, zsem.at[half, z], z=zz)

    og = [plane_gather(copies, obuf, g * 512, 512, g, gsem, coords) for g in range(2)]
    wg = [plane_gather(copies, wbuf, g * 1024, 1024, g, wsem, coords) for g in range(2)]

    def advance(gens):
        for gen in gens:
            next(gen)

    advance_state(0, 0, CHUNKS)
    finish_state(0)
    for load in loads[:5]:
        load.wait()
    pl.semaphore_wait(barrier, 2 * len(zs) + len(sends) + 1)
    send_y(0)
    advance(og)
    for zz in zs:
        copies(r_ref.at[:, pl.ds(pl.multiple_of(zz * 256 + t * 128, 128), 128)], rbuf.at[z], zsem.at[2, z], z=zz)
    for load in loads[5:]:
        load.start()
    advance(wg)
    rbuf[z] = r_ref[:, pl.ds(pl.multiple_of(z * 256 + t * 128, 128), 128)]
    advance_state(1, 0, CHUNKS)
    finish_state(1)
    send_y(1)
    advance(og)
    advance(og)
    for load in first[EARLY:]:
        load.wait()
    route[...] = jnp.zeros_like(route)
    route[0:6, :] = ids[...].astype(F32)
    route[8:14, :] = ew[...]
    route[16:20, :] = gw[...]
    row, tok = iota((2048, 128), 0), iota((2048, 128), 1)
    take = (row == (tok // 16) * 256 + q * 16 + tok % 16).astype(BF16)
    high, rest = split(route[...])
    mine = dot(high, take) + dot(rest, take)
    own = iota((16, 128), 0) + z * 16
    hit = jnp.zeros((16, 128), F32)
    weight = jnp.zeros((16, 128), F32)
    for k in range(6):
        same = mine[k : k + 1, :].astype(I32) == own
        hit = hit + same.astype(F32)
        weight = weight + jnp.where(same, mine[8 + k : 9 + k, :], 0.0)
    coarse = jnp.sum(jnp.where(iota((8, 128), 0) == z // 2, mine[16:24, :], 0.0), axis=0, keepdims=True)
    weight = weight * coarse
    a, b = iota((128, 128), 0), iota((128, 128), 1)
    before = ((a // 16 == b // 16) & (a < b)).astype(BF16)
    rank = dot(hit.astype(BF16), before)
    slot, tok3 = iota((16, 16, 128), 1), iota((16, 16, 128), 2)
    chosen = (
        (hit[:, None, :] > 0.5)
        & (rank[:, None, :] == (slot % 2).astype(F32))
        & (slot // 2 == tok3 // 16)
    )
    disp[...] = jnp.where(chosen, 1.0, 0.0).reshape(256, 128).astype(BF16)
    comb = jnp.where(chosen, jnp.broadcast_to(weight[:, None, :], (16, 16, 128)), 0.0).reshape(256, 128)
    comb = jnp.concatenate([comb[:128].T, comb[128:].T], axis=1)
    high, low = split(comb)
    c_hi[...] = high
    c_lo[...] = low

    advance(og)
    advance(og)
    advance(wg)
    advance(wg)
    advance(og)
    for half in range(2):
        for zz in zs[::-1]:
            copies.arrived(ybuf.at[zz, :, half * 512 : (half + 1) * 512], zsem.at[half, zz], z=zz)

    rows = ybuf[...].reshape(128, 1024)
    msend[...] = dot_t(rows, obuf[pl.ds(other * 8, 8)].reshape(128, 1024)).astype(BF16)
    copies(msend, mrecv, tsem.at[0], tp=other)
    mown[...] = dot_t(rows, obuf[pl.ds(t * 8, 8)].reshape(128, 1024))
    for zz in zs:
        copies.arrived(rbuf.at[zz], zsem.at[2, zz], z=zz)
    copies.arrived(mrecv, tsem.at[0], tp=other)
    mixed = mown[...] + mrecv[...].astype(F32)
    nbuf[z, t] = (rbuf[...].reshape(128, 128).astype(F32) + mixed).astype(BF16)
    for zz in zs:
        copies(nbuf.at[z, t], nbuf.at[z, t], zsem.at[3, z], z=zz)
    copies(nbuf.at[z, t], nbuf.at[z, t], nsem.at[z], tp=other)
    advance(wg)
    for i, zz in enumerate(zs):
        if i == 4:
            advance(wg)
        copies.arrived(nbuf.at[zz, t], zsem.at[3, zz], z=zz)
        copies(nbuf.at[zz, t], nbuf.at[zz, t], nsem.at[zz], tp=other)
    for load in loads[5:]:
        load.wait()
    for zz in [z] + zs:
        copies.arrived(nbuf.at[zz, other], nsem.at[zz], tp=other)

    for j in range(16):
        rn[:, j * 128 : (j + 1) * 128] = nbuf[j // 2, j % 2]
    wide = rn[...].astype(F32)
    scale = lax.rsqrt(jnp.mean(wide * wide, axis=-1, keepdims=True) + EPSILON)
    normed[...] = (wide * scale * gain[...]).astype(BF16)
    near = pl.ds(pl.multiple_of(t * 1024, 1024), 1024)
    far = pl.ds(pl.multiple_of(other * 1024, 1024), 1024)

    xsend[...] = dot(disp[...], normed[:, near]).astype(BF16).reshape(16, 16, 1024)
    for yy, xx in sends:
        copies(xsend.at[yy * 4 + xx], xfull.at[t, q], asem.at[0, q], y=yy, x=xx)
    xfull[t, q] = xsend[q]
    copies(xsend.at[q], xfull.at[t, q], fsem.at[q], tp=other)

    advance(wg)
    tokens = normed[...]
    vector = jnp.concatenate([bgate[j : j + 1, :].astype(F32) for j in range(16)], axis=1)
    score = jnp.sum(tokens.astype(F32) * vector, axis=-1, keepdims=True)
    gate = dot_t(tokens, wbuf[:, 0].reshape(256, 2048))
    lin = dot_t(tokens, wbuf[:, 1].reshape(256, 2048))
    hidden = (silu(gate) * lin / (1.0 + jnp.exp(-score))).astype(BF16)
    dsend[...] = dot(hidden, wbuf[:, 2, :, far].reshape(256, 1024)).astype(BF16)
    copies(dsend, drecv, tsem.at[1], tp=other)
    tot[...] = dot(hidden, wbuf[:, 2, :, near].reshape(256, 1024)).reshape(8, 16, 1024)

    def receive(w):
        for yy, xx, self in waves[w]:
            if not self:
                qq = yy * 4 + xx
                copies.arrived(xfull.at[t, qq], asem.at[0, qq], y=yy, x=xx)
                copies(xfull.at[t, qq], xfull.at[t, qq], fsem.at[qq], tp=other)

    def compute(w):
        places = [yy * 4 + xx for yy, xx, _ in waves[w]]
        for qq in places:
            copies.arrived(xfull.at[other, qq], fsem.at[qq], tp=other)
        left = jnp.concatenate([xfull[0, qq] for qq in places], axis=0)
        right = jnp.concatenate([xfull[1, qq] for qq in places], axis=0)
        gate = dot(left, eg[0:1024, :]) + dot(right, eg[1024:2048, :])
        lin = dot(left, eu[0:1024, :]) + dot(right, eu[1024:2048, :])
        hidden = (silu(gate) * lin).astype(BF16)
        esend[w] = dot(hidden, ed[:, far]).astype(BF16)
        copies(esend.at[w], erecv.at[w], tsem.at[4 + w], tp=other)
        emine[w] = dot(hidden, ed[:, near])

    def send_back(c, yy, xx):
        lanes = pl.ds(c * 512, 512)
        copies(csend.at[yy * 4 + xx, :, lanes], cbuf.at[q, :, lanes], asem.at[1 + c, q], y=yy, x=xx)

    def give_back(w):
        copies.arrived(erecv.at[w], tsem.at[4 + w], tp=other)
        done = (emine[w] + erecv[w].astype(F32)).astype(BF16)
        for i, (yy, xx, self) in enumerate(waves[w]):
            qq = yy * 4 + xx
            if self:
                cbuf[q] = done[i * 16 : (i + 1) * 16]
            else:
                csend[qq] = done[i * 16 : (i + 1) * 16]
                send_back(0, yy, xx)

    receive(0)
    receive(1)
    compute(0)
    receive(2)
    compute(1)
    give_back(0)
    receive(3)
    compute(2)
    give_back(1)
    compute(3)
    give_back(2)
    give_back(3)
    for w in range(4):
        for yy, xx, self in waves[w]:
            if not self:
                send_back(1, yy, xx)
    copies.arrived(drecv, tsem.at[1], tp=other)
    fin[...] = rn[pl.ds(pl.multiple_of(z * 16, 16), 16), :].astype(F32)
    for c in range(2):
        lanes = slice(c * 512, (c + 1) * 512)
        base = tot[:, :, lanes].reshape(128, 512) + drecv[:, lanes].astype(F32)
        for w in range(4):
            for yy, xx, self in waves[(w + 1) % 4 if w < 3 else 0]:
                if not self:
                    qq = yy * 4 + xx
                    copies.arrived(cbuf.at[qq, :, lanes], asem.at[1 + c, qq], y=yy, x=xx)
        back = cbuf[:, :, lanes].reshape(256, 512)
        total = base + dot(c_hi[...], back) + dot(c_lo[...], back)
        tot[:, :, lanes] = total.reshape(8, 16, 512)
        zsend[c] = total.reshape(8, 2, 8, 512).astype(BF16)
        for zz in zs:
            for tt in (t, other):
                copies(zsend.at[c, zz, tt], zrecv.at[c, z, t], rsem.at[c, z, t], z=zz, tp=tt)
        copies(zsend.at[c, z, other], zrecv.at[c, z, t], rsem.at[c, z, t], tp=other)
    for c in range(2):
        for side in (t, other):
            lanes = pl.ds(pl.multiple_of(side * 1024 + c * 512, 512), 512)
            final = fin[pl.ds(pl.multiple_of(t * 8, 8), 8), lanes]
            if side is t:
                final = final + tot[z, pl.ds(pl.multiple_of(t * 8, 8), 8), c * 512 : (c + 1) * 512]
            for zz in zs if side is t else [z] + zs:
                copies.arrived(zrecv.at[c, zz, side], rsem.at[c, zz, side], tp=other)
                final = final + zrecv[c, zz, side].astype(F32)
            out_ref[:, lanes] = final.astype(BF16)
    copies.drain()


def shards(resid, proj_x, proj_z, proj_bc, proj_dt, tail_x, tail_bc, taps_x, taps_bc, ssm_state, dt_bias, decay_log,
           group_gain, out_proj, ffn_gain, dense_gate, dense_up, dense_down, branch_gate, group_weights, expert_ids,
           expert_weights, exp_gate, exp_up, exp_down):
    small = (proj_x, proj_z, proj_bc, proj_dt, tail_x.transpose(1, 0, 2), tail_bc, taps_x, taps_bc, dt_bias.reshape(1, 16),
             decay_log.reshape(1, 16), group_gain.reshape(1, 1024), expert_ids.T, expert_weights.T, group_weights.T)
    vm = pl.BlockSpec(memory_space=VMEM)
    hbm = pl.BlockSpec(memory_space=pltpu.MemorySpace.HBM)
    scratch = [pltpu.VMEM(a.shape, a.dtype) for a in small]
    for shape, dtype in (
        ((32, 2048), F32), ((128, WIDE), BF16), ((2, 128, 128), F32), ((2, 128, 128), F32), ((2, 128, 128), F32),
        ((2, 128, 128), F32), ((2, 128, 128), F32), ((256, 128), BF16), ((128, 256), BF16), ((128, 256), BF16),
        ((16, 2048), BF16), ((1, 2048), F32), ((16, 128), BF16),
        ((16, 3, 16, 2048), BF16), ((16, 16, 1024), BF16), ((8, 16, 1024), BF16), ((8, 16, 128), BF16),
        ((128, 128), F32), ((128, 128), BF16), ((128, 128), BF16), ((8, 2, 128, 128), BF16), ((128, 2048), BF16),
        ((128, 2048), BF16), ((128, 1024), BF16), ((128, 1024), BF16), ((16, 16, 1024), BF16), ((2, 16, 16, 1024), BF16),
        ((4, 64, 1024), F32), ((4, 64, 1024), BF16), ((4, 64, 1024), BF16), ((16, 16, 1024), BF16), ((16, 16, 1024), BF16),
        ((8, 16, 1024), F32), ((2, 8, 2, 8, 512), BF16), ((2, 8, 2, 8, 512), BF16), ((16, 2048), F32),
        ((2048, 256), BF16), ((2048, 256), BF16), ((256, 2048), BF16),
    ):
        scratch.append(pltpu.VMEM(shape, dtype))
    for shape in ((224,), (2, 16, 2), (2, 16, 2), (4, 8), (3, 16), (8,), (8,), (16,), (2, 8, 2), (10,), (SMALL,), (2, CHUNKS)):
        scratch.append(pltpu.SemaphoreType.DMA(shape))
    new_state, out = pl.pallas_call(
        mesh_kernel,
        out_shape=(VMEM((16, 16, 4096), F32), VMEM((8, 2048), BF16)),
        in_specs=[hbm] * (SMALL + 11),
        out_specs=(vm, vm),
        scratch_shapes=scratch,
        compiler_params=pltpu.CompilerParams(collective_id=0, has_side_effects=True, vmem_limit_bytes=67_043_328 - (4200 << 10)),
        name="mesh",
    )(*small, ssm_state, resid, out_proj.T, dense_gate.T, dense_up.T, dense_down, ffn_gain.reshape(1, 2048),
      branch_gate.reshape(16, 128), exp_gate, exp_up, exp_down)
    return (out, new_state)


def solution(mesh):
    finer = Mesh(mesh.devices.reshape(NZ, NY, NX, mesh.shape["tp"]), EP_TP)
    in_specs = (
        P(EP, None), P(EP, "tp"), P(EP, "tp"), P(EP, None, "tp"), P(EP, "tp"), P(EP, None, "tp"), P(EP, None, None, "tp"),
        P(None, "tp"), P(None, None, "tp"), P(EP, "tp", None), P("tp"), P("tp"), P("tp"), P("tp", EP), P(),
        P(None, EP_TP), P(None, EP_TP), P(EP_TP, None), P(), P(), P(), P(), P(EP, None, "tp"), P(EP, None, "tp"),
        P(EP, "tp", None),
    )
    out_specs = (P(EP_TP, None), P(EP, "tp", None))
    return jax.shard_map(shards, mesh=finer, in_specs=in_specs, out_specs=out_specs, check_vma=False)
```

```python
import functools

import jax
import jax.numpy as jnp
from jax import lax
from jax.experimental import pallas as pl
from jax.experimental.pallas import tpu as pltpu
from jax.sharding import Mesh
from jax.sharding import PartitionSpec as P

F32, BF16, I32 = jnp.float32, jnp.bfloat16, jnp.int32
EP = ("z", "y", "x")
EP_TP = ("z", "y", "x", "tp")
NZ, NY, NX = 8, 4, 4
EPSILON = 1e-06
MESH = pl.DeviceIdType.MESH
VMEM = pltpu.MemorySpace.VMEM
CHUNKS = 4
WIDE = 4096 // CHUNKS
EARLY = 11
PARTS = 2
PART = 1024 // PARTS
SMALL = 14


def dot(a, b):
    return lax.dot_general(a, b, (((1,), (0,)), ((), ())), preferred_element_type=F32)


def dot_t(a, b):
    return lax.dot_general(a, b, (((1,), (1,)), ((), ())), preferred_element_type=F32)


def silu(v):
    return v / (1.0 + jnp.exp(-v))


def iota(shape, dim):
    return lax.broadcasted_iota(I32, shape, dim)


def split(v):
    high = v.astype(BF16)
    return high, (v - high.astype(F32)).astype(BF16)


def spread(v):
    total = v.shape[1]
    per = 8 // (total // 64)
    mask = (iota((8, total), 1) // 64) == (iota((8, total), 0) // per)
    rows = jnp.where(mask[None], jnp.broadcast_to(v[:, None, :], (16, 8, total)), 0.0).reshape(128, total)
    pick = ((iota((total, 128), 0) % 64) == (iota((total, 128), 1) % 64)).astype(BF16)
    high, low = split(rows)
    return dot(high, pick) + dot(low, pick)


def column(v, half):
    mine = (iota((8, 16), 1) == iota((8, 16), 0) + half * 8)[None]
    wide = jnp.where(mine, jnp.broadcast_to(v[:, None, :], (16, 8, 16)), 0.0)
    return jnp.sum(wide, axis=-1, keepdims=True).reshape(128, 1)


class Copies:
    def __init__(self, sems):
        self.sems, self.started = sems, []

    def __call__(self, src, dst, recv, **where):
        copy = pltpu.make_async_remote_copy(
            src_ref=src, dst_ref=dst, send_sem=self.sems.at[len(self.started)], recv_sem=recv,
            device_id=where, device_id_type=MESH,
        )
        copy.start()
        self.started.append(copy)

    def arrived(self, ref, recv, **where):
        pltpu.make_async_remote_copy(
            src_ref=ref, dst_ref=ref, send_sem=self.sems.at[0], recv_sem=recv, device_id=where, device_id_type=MESH,
        ).wait_recv()

    def drain(self):
        for copy in self.started:
            copy.wait_send()


def plane_gather(copies, buf, lane, width, g, rsem, coords):
    fa, sa = ("x", "y") if g == 0 else ("y", "x")
    f, s = coords[fa], coords[sa]

    def place(df, ds):
        fv, sv = lax.rem(f + df + 4, 4), lax.rem(s + ds + 4, 4)
        return sv * 4 + fv if g == 0 else fv * 4 + sv

    def piece(qi, part):
        start, size = (lane, width) if part == 0 else (lane + (part - 1) * (width // 2), width // 2)
        lead = (qi,) + (slice(None),) * (len(buf.shape) - 2)
        return buf.at[lead + (pl.ds(start, size),)]

    def send(df, ds, part, axis, move):
        qi = place(df, ds)
        ref = piece(qi, part)
        copies(ref, ref, rsem.at[g, qi, 1 if part == 2 else 0], **{axis: lax.rem(coords[axis] + move + 4, 4)})

    def wait(df, ds, part):
        qi = place(df, ds)
        copies.arrived(piece(qi, part), rsem.at[g, qi, 1 if part == 2 else 0], **{fa: lax.rem(f + 1, 4)})

    turns = ((-1, 1), (1, 2))
    for axis in (fa, sa):
        for move in (1, -1):
            send(0, 0, 0, axis, move)
    yield
    for df, part in turns:
        wait(df, 0, 0)
        send(df, 0, part, fa, -df)
    for ds, part in turns:
        wait(0, ds, 0)
        send(0, ds, part, sa, -ds)
    yield
    for df in (-1, 1):
        for move in (1, -1):
            send(df, 0, 0, sa, move)
    yield
    wait(2, 0, 1)
    wait(2, 0, 2)
    for move in (1, -1):
        send(2, 0, 0, sa, move)
    yield
    for df in (-1, 1):
        for ds, part in turns:
            wait(df, ds, 0)
            send(df, ds, part, sa, -ds)
    yield
    for ds, part in turns:
        wait(2, ds, 0)
        send(2, ds, part, sa, -ds)
    yield
    for df in (0, -1, 1, 2):
        wait(df, 2, 1)
        wait(df, 2, 2)
    yield


Z_ORDER = (4, 3, 5, 2, 6, 1, 7)
SENDS = ((2, 2), (2, 1), (2, 3), (2, 0), (1, 2), (1, 1), (1, 3), (1, 0), (3, 2), (3, 1), (3, 3), (3, 0), (0, 2), (0, 1), (0, 3))
WAVES = ((2, 3), (1, 0))


def mesh_kernel(*refs):
    small, (state, r_hbm, ot_hbm, gt_hbm, ut_hbm, dn_hbm, gain_hbm, bg_hbm, eg_hbm, eu_hbm, ed_hbm) = refs[:SMALL], refs[SMALL : SMALL + 11]
    new_state, out_ref = refs[SMALL + 11 : SMALL + 13]
    refs = refs[SMALL + 13 :]
    px, pz, pb, pdt, tx, tb, wx, wb, dtb, dlg, gg, ids, ew, gw = refs[:SMALL]
    (route, grid, xs_s, in_s, rd_s, de_s, rdo, disp, c_hi, c_lo, r_ref, gain, bgate,
     wbuf, obuf, ybuf, rbuf, mown, msend, mrecv, nbuf, rn, normed, dsend, drecv, xsend, xfull, emine, esend, erecv,
     csend, cbuf, tot, zsend, zrecv, fin, eg, eu, ed,
     ssem, wsem, gsem, zsem, asem, tsem, nsem, fsem, rsem, lsem, msem, isem) = refs[SMALL:]
    z, y, x, t = (lax.axis_index(a) for a in EP_TP)
    coords = {"x": x, "y": y}
    q = y * 4 + x
    other = 1 - t
    sends = [(lax.rem(y + dy, 4), lax.rem(x + dx, 4)) for dy, dx in SENDS]
    waves = [[(lax.rem(y + dy, 4), lax.rem(x + dx, 4), dy == 0 and dx == 0) for dy in wave for dx in (2, 3, 1, 0)] for wave in WAVES]
    zs = [lax.rem(z + d, 8) for d in Z_ORDER]

    barrier = pltpu.get_barrier_semaphore()
    for zz in zs:
        pl.semaphore_signal(barrier, inc=1, device_id={"z": zz}, device_id_type=MESH)
    for yy, xx in sends:
        pl.semaphore_signal(barrier, inc=1, device_id={"y": yy, "x": xx}, device_id_type=MESH)
    pl.semaphore_signal(barrier, inc=1, device_id={"tp": other}, device_id_type=MESH)
    for zz in zs:
        pl.semaphore_signal(barrier, inc=1, device_id={"z": zz, "tp": other}, device_id_type=MESH)

    def block(ref, half, j):
        return ref.at[:, pl.ds(half * 8, 8), pl.ds(j * WIDE, WIDE)]

    def in_copy(half, j):
        return pltpu.make_async_copy(block(state, half, j), block(new_state, half, j), isem.at[half, j])

    first = [pltpu.make_async_copy(src, dst, msem.at[i]) for i, (src, dst) in enumerate(zip(small, refs[:SMALL]))]
    for load in first[:EARLY]:
        load.start()
    for j in range(CHUNKS):
        in_copy(0, j).start()
    pairs = ((ot_hbm, obuf.at[y, x]), (gt_hbm, wbuf.at[q, 0]), (ut_hbm, wbuf.at[q, 1]), (dn_hbm, wbuf.at[q, 2]), (r_hbm, r_ref),
             (gain_hbm, gain), (bg_hbm, bgate), (eg_hbm.at[0], eg), (eu_hbm.at[0], eu), (ed_hbm.at[0], ed))
    loads = [pltpu.make_async_copy(src, dst, lsem.at[i]) for i, (src, dst) in enumerate(pairs)]
    grid[...] = ((iota((128, WIDE), 0) % 64) == (iota((128, WIDE), 1) // 64)).astype(BF16)
    for load in first[:EARLY]:
        load.wait()
    for j in range(CHUNKS):
        in_copy(1, j).start()
    for load in loads[:5] + first[EARLY:]:
        load.start()

    conv_x = px[...].astype(F32) * wx[3:4, :].astype(F32)
    for w in range(3):
        conv_x = conv_x + tx[w].astype(F32) * wx[w : w + 1, :].astype(F32)
    conv_x = silu(conv_x)
    conv_bc = pb[...].astype(F32) * wb[3:4].astype(F32)
    for w in range(3):
        conv_bc = conv_bc + tb[:, w].astype(F32) * wb[w : w + 1].astype(F32)
    conv_bc = silu(conv_bc)
    top = iota((16, 2, 256), 1) == 0
    inputs = jnp.sum(jnp.where(top, conv_bc, 0.0), axis=1)
    reads = jnp.sum(jnp.where(top, 0.0, conv_bc), axis=1)
    pre = pdt[...].astype(F32) + dtb[...]
    step = jnp.maximum(pre, 0.0) + jnp.log1p(jnp.exp(-jnp.abs(pre)))
    decay = jnp.exp(-step * jnp.exp(dlg[...]))
    for half in range(2):
        x_rows = spread(conv_x[:, half * 512 : (half + 1) * 512]) * column(step, half)
        high, low = split(x_rows)
        xs_s[half] = jnp.where(iota((128, 128), 1) < 64, high.astype(F32), low.astype(F32))
        in_s[half] = spread(inputs[:, half * 128 : (half + 1) * 128])
        rd_s[half] = spread(reads[:, half * 128 : (half + 1) * 128])
        de_s[half] = jnp.broadcast_to(column(decay, half), (128, 128))

    def advance_state(half, low, high):
        lanes = WIDE // 64
        for j in range(low, high):
            in_copy(half, j).wait()
        total = None
        for j in range(low, high):
            here = (slice(None), slice(half * 8, half * 8 + 8), slice(j * WIDE, (j + 1) * WIDE))
            shifted = xs_s[half] if j == 0 else pltpu.roll(xs_s[half], 128 - j * lanes, 1)
            fresh = dot(shifted.astype(BF16), grid[...])
            new = jnp.tile(de_s[half], (1, WIDE // 128)) * new_state[here].reshape(128, WIDE) + fresh * jnp.tile(in_s[half], (1, WIDE // 128))
            new_state[here] = new.reshape(16, 8, WIDE)
            part = dot_t((new * jnp.tile(rd_s[half], (1, WIDE // 128))).astype(BF16), grid[...])
            part = part if j == 0 else pltpu.roll(part, j * lanes, 1)
            total = part if total is None else total + part
        rdo[half] = total if low == 0 else rdo[half] + total

    def finish_state(half):
        keep = (iota((8, 512), 1) // 64) == iota((8, 512), 0)
        wide = jnp.tile(rdo[half], (1, 4)).reshape(16, 8, 512)
        read = jnp.sum(jnp.where(keep[None], wide, 0.0), axis=1)
        gated = read * silu(pz[:, half * 512 : (half + 1) * 512].astype(F32))
        for g in range(2):
            lanes = slice(half * 512 + g * 256, half * 512 + (g + 1) * 256)
            part = gated[:, g * 256 : (g + 1) * 256]
            scale = lax.rsqrt(jnp.mean(part * part, axis=-1, keepdims=True) + EPSILON)
            ybuf[z, :, lanes] = (part * scale * gg[:, lanes]).astype(BF16)

    copies = Copies(ssem)

    def send_y(half):
        ref = ybuf.at[z, :, half * 512 : (half + 1) * 512]
        for zz in zs:
            copies(ref, ref, zsem.at[half, z], z=zz)

    wg = [plane_gather(copies, wbuf, g * 1024, 1024, g, wsem, coords) for g in range(2)]

    def advance(gens):
        for gen in gens:
            next(gen)

    advance_state(0, 0, CHUNKS)
    finish_state(0)
    for load in loads[:5]:
        load.wait()
    pl.semaphore_wait(barrier, 2 * len(zs) + len(sends) + 1)
    send_y(0)
    for yy, xx in sends:
        copies(obuf.at[y, x], obuf.at[y, x], gsem.at[q], y=yy, x=xx)
    for zz in zs:
        copies(r_ref.at[:, pl.ds(pl.multiple_of(zz * 256 + t * 128, 128), 128)], rbuf.at[z], zsem.at[2, z], z=zz)
    advance(wg)
    for load in loads[5:]:
        load.start()
    rbuf[z] = r_ref[:, pl.ds(pl.multiple_of(z * 256 + t * 128, 128), 128)]
    advance_state(1, 0, CHUNKS)
    finish_state(1)
    send_y(1)
    for load in first[EARLY:]:
        load.wait()
    route[...] = jnp.zeros_like(route)
    route[0:6, :] = ids[...].astype(F32)
    route[8:14, :] = ew[...]
    route[16:20, :] = gw[...]
    row, tok = iota((2048, 128), 0), iota((2048, 128), 1)
    take = (row == (tok // 16) * 256 + q * 16 + tok % 16).astype(BF16)
    high, rest = split(route[...])
    mine = dot(high, take) + dot(rest, take)
    expert = iota((16, 128), 0) + z * 16
    hit = jnp.zeros((16, 128), F32)
    weight = jnp.zeros((16, 128), F32)
    for k in range(6):
        same = mine[k : k + 1, :].astype(I32) == expert
        hit = hit + same.astype(F32)
        weight = weight + jnp.where(same, mine[8 + k : 9 + k, :], 0.0)
    coarse = jnp.sum(jnp.where(iota((8, 128), 0) == z // 2, mine[16:24, :], 0.0), axis=0, keepdims=True)
    weight = weight * coarse
    a, b = iota((128, 128), 0), iota((128, 128), 1)
    before = ((a // 16 == b // 16) & (a < b)).astype(BF16)
    rank = dot(hit.astype(BF16), before)
    slot, tok3 = iota((16, 16, 128), 1), iota((16, 16, 128), 2)
    chosen = (
        (hit[:, None, :] > 0.5)
        & (rank[:, None, :] == (slot % 2).astype(F32))
        & (slot // 2 == tok3 // 16)
    )
    disp[...] = jnp.where(chosen, 1.0, 0.0).reshape(256, 128).astype(BF16)
    comb = jnp.where(chosen, jnp.broadcast_to(weight[:, None, :], (16, 16, 128)), 0.0).reshape(256, 128)
    comb = jnp.concatenate([comb[:128].T, comb[128:].T], axis=1)
    high, low = split(comb)
    c_hi[...] = high
    c_lo[...] = low

    for half in range(2):
        for zz in zs[::-1]:
            copies.arrived(ybuf.at[zz, :, half * 512 : (half + 1) * 512], zsem.at[half, zz], z=zz)

    for yy, xx in sends:
        copies.arrived(obuf.at[yy, xx], gsem.at[yy * 4 + xx], y=yy, x=xx)
    rows = ybuf[...].reshape(128, 1024)
    msend[...] = dot_t(rows, obuf[pl.ds(other * 2, 2)].reshape(128, 1024)).astype(BF16)
    copies(msend, mrecv, tsem.at[0], tp=other)
    mown[...] = dot_t(rows, obuf[pl.ds(t * 2, 2)].reshape(128, 1024))
    for zz in zs:
        copies.arrived(rbuf.at[zz], zsem.at[2, zz], z=zz)
    copies.arrived(mrecv, tsem.at[0], tp=other)
    mixed = mown[...] + mrecv[...].astype(F32)
    nbuf[z, t] = (rbuf[...].reshape(128, 128).astype(F32) + mixed).astype(BF16)
    for zz in zs:
        copies(nbuf.at[z, t], nbuf.at[z, t], zsem.at[3, z], z=zz)
    copies(nbuf.at[z, t], nbuf.at[z, t], nsem.at[z], tp=other)
    advance(wg)
    advance(wg)
    advance(wg)
    for i, zz in enumerate(zs):
        copies.arrived(nbuf.at[zz, t], zsem.at[3, zz], z=zz)
        copies(nbuf.at[zz, t], nbuf.at[zz, t], nsem.at[zz], tp=other)
    for load in loads[5:]:
        load.wait()
    for zz in [z] + zs:
        copies.arrived(nbuf.at[zz, other], nsem.at[zz], tp=other)

    for j in range(16):
        rn[:, j * 128 : (j + 1) * 128] = nbuf[j // 2, j % 2]
    wide = rn[...].astype(F32)
    scale = lax.rsqrt(jnp.mean(wide * wide, axis=-1, keepdims=True) + EPSILON)
    normed[...] = (wide * scale * gain[...]).astype(BF16)
    near = pl.ds(pl.multiple_of(t * 1024, 1024), 1024)
    far = pl.ds(pl.multiple_of(other * 1024, 1024), 1024)

    xsend[...] = dot(disp[...], normed[:, near]).astype(BF16).reshape(16, 16, 1024)
    for yy, xx in sends:
        copies(xsend.at[yy * 4 + xx], xfull.at[t, q], asem.at[0, q], y=yy, x=xx)
    xfull[t, q] = xsend[q]
    copies(xsend.at[q], xfull.at[t, q], fsem.at[q], tp=other)

    advance(wg)
    advance(wg)

    def receive(w):
        for yy, xx, self in waves[w]:
            if not self:
                qq = yy * 4 + xx
                copies.arrived(xfull.at[t, qq], asem.at[0, qq], y=yy, x=xx)
                copies(xfull.at[t, qq], xfull.at[t, qq], fsem.at[qq], tp=other)

    def compute(w):
        places = [yy * 4 + xx for yy, xx, _ in waves[w]]
        for qq in places:
            copies.arrived(xfull.at[other, qq], fsem.at[qq], tp=other)
        left = jnp.concatenate([xfull[0, qq] for qq in places], axis=0)
        right = jnp.concatenate([xfull[1, qq] for qq in places], axis=0)
        gate = dot(left, eg[0:1024, :]) + dot(right, eg[1024:2048, :])
        lin = dot(left, eu[0:1024, :]) + dot(right, eu[1024:2048, :])
        hidden = (silu(gate) * lin).astype(BF16)
        esend[w] = dot(hidden, ed[:, far]).astype(BF16)
        copies(esend.at[w], erecv.at[w], tsem.at[4 + w], tp=other)
        emine[w] = dot(hidden, ed[:, near])

    def send_back(c, yy, xx):
        lanes = pl.ds(c * PART, PART)
        copies(csend.at[yy * 4 + xx, :, lanes], cbuf.at[q, :, lanes], asem.at[1 + c, q], y=yy, x=xx)

    def give_back(w):
        copies.arrived(erecv.at[w], tsem.at[4 + w], tp=other)
        done = (emine[w] + erecv[w].astype(F32)).astype(BF16)
        for i, (yy, xx, self) in enumerate(waves[w]):
            qq = yy * 4 + xx
            if self:
                cbuf[q] = done[i * 16 : (i + 1) * 16]
            else:
                csend[qq] = done[i * 16 : (i + 1) * 16]
                send_back(0, yy, xx)

    receive(0)
    receive(1)
    compute(0)
    compute(1)
    give_back(0)
    give_back(1)
    for c in range(1, PARTS):
        for wave in waves:
            for yy, xx, self in wave:
                if not self:
                    send_back(c, yy, xx)
    advance(wg)
    tokens = normed[...]
    vector = jnp.concatenate([bgate[j : j + 1, :].astype(F32) for j in range(16)], axis=1)
    score = jnp.sum(tokens.astype(F32) * vector, axis=-1, keepdims=True)
    gate = dot_t(tokens, wbuf[:, 0].reshape(256, 2048))
    lin = dot_t(tokens, wbuf[:, 1].reshape(256, 2048))
    hidden = (silu(gate) * lin / (1.0 + jnp.exp(-score))).astype(BF16)
    dsend[...] = dot(hidden, wbuf[:, 2, :, far].reshape(256, 1024)).astype(BF16)
    copies(dsend, drecv, tsem.at[1], tp=other)
    tot[...] = dot(hidden, wbuf[:, 2, :, near].reshape(256, 1024)).reshape(8, 16, 1024)

    copies.arrived(drecv, tsem.at[1], tp=other)
    fin[...] = rn[pl.ds(pl.multiple_of(z * 16, 16), 16), :].astype(F32)
    for c in range(PARTS):
        lanes = slice(c * PART, (c + 1) * PART)
        base = tot[:, :, lanes].reshape(128, PART) + drecv[:, lanes].astype(F32)
        for wave in waves:
            for yy, xx, self in wave:
                if not self:
                    qq = yy * 4 + xx
                    copies.arrived(cbuf.at[qq, :, lanes], asem.at[1 + c, qq], y=yy, x=xx)
        back = cbuf[:, :, lanes].reshape(256, PART)
        total = base + dot(c_hi[...], back) + dot(c_lo[...], back)
        tot[:, :, lanes] = total.reshape(8, 16, PART)
        zsend[c] = total.reshape(8, 2, 8, PART).astype(BF16)
        for zz in zs:
            for tt in (t, other):
                copies(zsend.at[c, zz, tt], zrecv.at[c, z, t], rsem.at[c, z, t], z=zz, tp=tt)
        copies(zsend.at[c, z, other], zrecv.at[c, z, t], rsem.at[c, z, t], tp=other)
    for c in range(PARTS):
        for side in (t, other):
            lanes = pl.ds(pl.multiple_of(side * 1024 + c * PART, PART), PART)
            final = fin[pl.ds(pl.multiple_of(t * 8, 8), 8), lanes]
            if side is t:
                final = final + tot[z, pl.ds(pl.multiple_of(t * 8, 8), 8), c * PART : (c + 1) * PART]
            for zz in zs if side is t else [z] + zs:
                copies.arrived(zrecv.at[c, zz, side], rsem.at[c, zz, side], tp=other)
                final = final + zrecv[c, zz, side].astype(F32)
            out_ref[:, lanes] = final.astype(BF16)
    copies.drain()


def shards(resid, proj_x, proj_z, proj_bc, proj_dt, tail_x, tail_bc, taps_x, taps_bc, ssm_state, dt_bias, decay_log,
           group_gain, out_proj, ffn_gain, dense_gate, dense_up, dense_down, branch_gate, group_weights, expert_ids,
           expert_weights, exp_gate, exp_up, exp_down):
    small = (proj_x, proj_z, proj_bc, proj_dt, tail_x.transpose(1, 0, 2), tail_bc, taps_x, taps_bc, dt_bias.reshape(1, 16),
             decay_log.reshape(1, 16), group_gain.reshape(1, 1024), expert_ids.T, expert_weights.T, group_weights.T)
    vm = pl.BlockSpec(memory_space=VMEM)
    hbm = pl.BlockSpec(memory_space=pltpu.MemorySpace.HBM)
    scratch = [pltpu.VMEM(a.shape, a.dtype) for a in small]
    for shape, dtype in (
        ((32, 2048), F32), ((128, WIDE), BF16), ((2, 128, 128), F32), ((2, 128, 128), F32), ((2, 128, 128), F32),
        ((2, 128, 128), F32), ((2, 128, 128), F32), ((256, 128), BF16), ((128, 256), BF16), ((128, 256), BF16),
        ((16, 2048), BF16), ((1, 2048), F32), ((16, 128), BF16),
        ((16, 3, 16, 2048), BF16), ((4, 4, 16, 1024), BF16), ((8, 16, 1024), BF16), ((8, 16, 128), BF16),
        ((128, 128), F32), ((128, 128), BF16), ((128, 128), BF16), ((8, 2, 128, 128), BF16), ((128, 2048), BF16),
        ((128, 2048), BF16), ((128, 1024), BF16), ((128, 1024), BF16), ((16, 16, 1024), BF16), ((2, 16, 16, 1024), BF16),
        ((2, 128, 1024), F32), ((2, 128, 1024), BF16), ((2, 128, 1024), BF16), ((16, 16, 1024), BF16), ((16, 16, 1024), BF16),
        ((8, 16, 1024), F32), ((PARTS, 8, 2, 8, PART), BF16), ((PARTS, 8, 2, 8, PART), BF16), ((16, 2048), F32),
        ((2048, 256), BF16), ((2048, 256), BF16), ((256, 2048), BF16),
    ):
        scratch.append(pltpu.VMEM(shape, dtype))
    for shape in ((160 + 45 * PARTS,), (2, 16, 2), (16,), (4, 8), (1 + PARTS, 16), (8,), (8,), (16,), (PARTS, 8, 2), (10,), (SMALL,), (2, CHUNKS)):
        scratch.append(pltpu.SemaphoreType.DMA(shape))
    new_state, out = pl.pallas_call(
        mesh_kernel,
        out_shape=(VMEM((16, 16, 4096), F32), VMEM((8, 2048), BF16)),
        in_specs=[hbm] * (SMALL + 11),
        out_specs=(vm, vm),
        scratch_shapes=scratch,
        compiler_params=pltpu.CompilerParams(collective_id=0, has_side_effects=True, vmem_limit_bytes=67_043_328 - (4200 << 10)),
        name="mesh",
    )(*small, ssm_state, resid, out_proj.T, dense_gate.T, dense_up.T, dense_down, ffn_gain.reshape(1, 2048),
      branch_gate.reshape(16, 128), exp_gate, exp_up, exp_down)
    return (out, new_state)


def solution(mesh):
    finer = Mesh(mesh.devices.reshape(NZ, NY, NX, mesh.shape["tp"]), EP_TP)
    in_specs = (
        P(EP, None), P(EP, "tp"), P(EP, "tp"), P(EP, None, "tp"), P(EP, "tp"), P(EP, None, "tp"), P(EP, None, None, "tp"),
        P(None, "tp"), P(None, None, "tp"), P(EP, "tp", None), P("tp"), P("tp"), P("tp"), P("tp", EP), P(),
        P(None, EP_TP), P(None, EP_TP), P(EP_TP, None), P(), P(), P(), P(), P(EP, None, "tp"), P(EP, None, "tp"),
        P(EP, "tp", None),
    )
    out_specs = (P(EP_TP, None), P(EP, "tp", None))
    return jax.shard_map(shards, mesh=finer, in_specs=in_specs, out_specs=out_specs, check_vma=False)
```

```python
import functools

import jax
import jax.numpy as jnp
from jax import lax
from jax.experimental import pallas as pl
from jax.experimental.pallas import tpu as pltpu
from jax.sharding import Mesh
from jax.sharding import PartitionSpec as P

F32, BF16, I32 = jnp.float32, jnp.bfloat16, jnp.int32
EP = ("z", "y", "x")
EP_TP = ("z", "y", "x", "tp")
NZ, NY, NX = 8, 4, 4
EPSILON = 1e-06
MESH = pl.DeviceIdType.MESH
VMEM = pltpu.MemorySpace.VMEM
CHUNKS = 4
WIDE = 4096 // CHUNKS
EARLY = 11
PARTS = 2
PART = 1024 // PARTS
SMALL = 14


def dot(a, b):
    return lax.dot_general(a, b, (((1,), (0,)), ((), ())), preferred_element_type=F32)


def dot_t(a, b):
    return lax.dot_general(a, b, (((1,), (1,)), ((), ())), preferred_element_type=F32)


def silu(v):
    return v / (1.0 + jnp.exp(-v))


def iota(shape, dim):
    return lax.broadcasted_iota(I32, shape, dim)


def split(v):
    high = v.astype(BF16)
    return high, (v - high.astype(F32)).astype(BF16)


def spread(v):
    total = v.shape[1]
    per = 8 // (total // 64)
    mask = (iota((8, total), 1) // 64) == (iota((8, total), 0) // per)
    rows = jnp.where(mask[None], jnp.broadcast_to(v[:, None, :], (16, 8, total)), 0.0).reshape(128, total)
    pick = ((iota((total, 128), 0) % 64) == (iota((total, 128), 1) % 64)).astype(BF16)
    high, low = split(rows)
    return dot(high, pick) + dot(low, pick)


def column(v, half):
    mine = (iota((8, 16), 1) == iota((8, 16), 0) + half * 8)[None]
    wide = jnp.where(mine, jnp.broadcast_to(v[:, None, :], (16, 8, 16)), 0.0)
    return jnp.sum(wide, axis=-1, keepdims=True).reshape(128, 1)


class Copies:
    def __init__(self, sems):
        self.sems, self.started = sems, []

    def __call__(self, src, dst, recv, **where):
        copy = pltpu.make_async_remote_copy(
            src_ref=src, dst_ref=dst, send_sem=self.sems.at[len(self.started)], recv_sem=recv,
            device_id=where, device_id_type=MESH,
        )
        copy.start()
        self.started.append(copy)

    def arrived(self, ref, recv, **where):
        pltpu.make_async_remote_copy(
            src_ref=ref, dst_ref=ref, send_sem=self.sems.at[0], recv_sem=recv, device_id=where, device_id_type=MESH,
        ).wait_recv()

    def drain(self):
        for copy in self.started:
            copy.wait_send()


def plane_gather(copies, buf, lane, width, g, rsem, coords):
    fa, sa = ("x", "y") if g == 0 else ("y", "x")
    f, s = coords[fa], coords[sa]

    def place(df, ds):
        fv, sv = lax.rem(f + df + 4, 4), lax.rem(s + ds + 4, 4)
        return sv * 4 + fv if g == 0 else fv * 4 + sv

    def piece(qi, part):
        start, size = (lane, width) if part == 0 else (lane + (part - 1) * (width // 2), width // 2)
        lead = (qi,) + (slice(None),) * (len(buf.shape) - 2)
        return buf.at[lead + (pl.ds(start, size),)]

    def send(df, ds, part, axis, move):
        qi = place(df, ds)
        ref = piece(qi, part)
        copies(ref, ref, rsem.at[g, qi, 1 if part == 2 else 0], **{axis: lax.rem(coords[axis] + move + 4, 4)})

    def wait(df, ds, part):
        qi = place(df, ds)
        copies.arrived(piece(qi, part), rsem.at[g, qi, 1 if part == 2 else 0], **{fa: lax.rem(f + 1, 4)})

    turns = ((-1, 1), (1, 2))
    for axis in (fa, sa):
        for move in (1, -1):
            send(0, 0, 0, axis, move)
    yield
    for df, part in turns:
        wait(df, 0, 0)
        send(df, 0, part, fa, -df)
    for ds, part in turns:
        wait(0, ds, 0)
        send(0, ds, part, sa, -ds)
    yield
    for df in (-1, 1):
        for move in (1, -1):
            send(df, 0, 0, sa, move)
    yield
    wait(2, 0, 1)
    wait(2, 0, 2)
    for move in (1, -1):
        send(2, 0, 0, sa, move)
    yield
    for df in (-1, 1):
        for ds, part in turns:
            wait(df, ds, 0)
            send(df, ds, part, sa, -ds)
    yield
    for ds, part in turns:
        wait(2, ds, 0)
        send(2, ds, part, sa, -ds)
    yield
    for df in (0, -1, 1, 2):
        wait(df, 2, 1)
        wait(df, 2, 2)
    yield


Z_ORDER = (4, 3, 5, 2, 6, 1, 7)
SENDS = ((2, 2), (2, 1), (2, 3), (2, 0), (1, 2), (1, 1), (1, 3), (1, 0), (3, 2), (3, 1), (3, 3), (3, 0), (0, 2), (0, 1), (0, 3))
WAVES = ((2, 3), (1, 0))


def mesh_kernel(*refs):
    small, (state, r_hbm, ot_hbm, gt_hbm, ut_hbm, dn_hbm, gain_hbm, bg_hbm, eg_hbm, eu_hbm, ed_hbm) = refs[:SMALL], refs[SMALL : SMALL + 11]
    new_state, out_ref = refs[SMALL + 11 : SMALL + 13]
    refs = refs[SMALL + 13 :]
    px, pz, pb, pdt, tx, tb, wx, wb, dtb, dlg, gg, ids, ew, gw = refs[:SMALL]
    (route, grid, xs_s, in_s, rd_s, de_s, rdo, disp, c_hi, c_lo, r_ref, gain, bgate,
     wbuf, obuf, ybuf, rbuf, mown, msend, mrecv, nbuf, rn, normed, dsend, drecv, xsend, xfull, emine, esend, erecv,
     csend, cbuf, tot, zsend, zrecv, fin, eg, eu, ed,
     ssem, wsem, gsem, zsem, asem, tsem, nsem, fsem, rsem, lsem, msem, isem) = refs[SMALL:]
    z, y, x, t = (lax.axis_index(a) for a in EP_TP)
    coords = {"x": x, "y": y}
    q = y * 4 + x
    other = 1 - t
    sends = [(lax.rem(y + dy, 4), lax.rem(x + dx, 4)) for dy, dx in SENDS]
    waves = [[(lax.rem(y + dy, 4), lax.rem(x + dx, 4), dy == 0 and dx == 0) for dy in wave for dx in (2, 3, 1, 0)] for wave in WAVES]
    zs = [lax.rem(z + d, 8) for d in Z_ORDER]

    barrier = pltpu.get_barrier_semaphore()
    for zz in zs:
        pl.semaphore_signal(barrier, inc=1, device_id={"z": zz}, device_id_type=MESH)
    for yy, xx in sends:
        pl.semaphore_signal(barrier, inc=1, device_id={"y": yy, "x": xx}, device_id_type=MESH)
    pl.semaphore_signal(barrier, inc=1, device_id={"tp": other}, device_id_type=MESH)
    for zz in zs:
        pl.semaphore_signal(barrier, inc=1, device_id={"z": zz, "tp": other}, device_id_type=MESH)

    def block(ref, half, j):
        return ref.at[:, pl.ds(half * 8, 8), pl.ds(j * WIDE, WIDE)]

    def in_copy(half, j):
        return pltpu.make_async_copy(block(state, half, j), block(new_state, half, j), isem.at[half, j])

    first = [pltpu.make_async_copy(src, dst, msem.at[i]) for i, (src, dst) in enumerate(zip(small, refs[:SMALL]))]
    for load in first[:EARLY]:
        load.start()
    for j in range(CHUNKS):
        in_copy(0, j).start()
    pairs = ((ot_hbm, obuf.at[y, x]), (gt_hbm, wbuf.at[q, 0]), (ut_hbm, wbuf.at[q, 1]), (dn_hbm, wbuf.at[q, 2]), (r_hbm, r_ref),
             (gain_hbm, gain), (bg_hbm, bgate), (eg_hbm.at[0], eg), (eu_hbm.at[0], eu), (ed_hbm.at[0], ed))
    loads = [pltpu.make_async_copy(src, dst, lsem.at[i]) for i, (src, dst) in enumerate(pairs)]
    grid[...] = ((iota((128, WIDE), 0) % 64) == (iota((128, WIDE), 1) // 64)).astype(BF16)
    for load in first[:EARLY]:
        load.wait()
    for j in range(CHUNKS):
        in_copy(1, j).start()
    for load in loads[:5] + first[EARLY:]:
        load.start()

    conv_x = px[...].astype(F32) * wx[3:4, :].astype(F32)
    for w in range(3):
        conv_x = conv_x + tx[w].astype(F32) * wx[w : w + 1, :].astype(F32)
    conv_x = silu(conv_x)
    conv_bc = pb[...].astype(F32) * wb[3:4].astype(F32)
    for w in range(3):
        conv_bc = conv_bc + tb[:, w].astype(F32) * wb[w : w + 1].astype(F32)
    conv_bc = silu(conv_bc)
    top = iota((16, 2, 256), 1) == 0
    inputs = jnp.sum(jnp.where(top, conv_bc, 0.0), axis=1)
    reads = jnp.sum(jnp.where(top, 0.0, conv_bc), axis=1)
    pre = pdt[...].astype(F32) + dtb[...]
    step = jnp.maximum(pre, 0.0) + jnp.log1p(jnp.exp(-jnp.abs(pre)))
    decay = jnp.exp(-step * jnp.exp(dlg[...]))
    for half in range(2):
        x_rows = spread(conv_x[:, half * 512 : (half + 1) * 512]) * column(step, half)
        high, low = split(x_rows)
        xs_s[half] = jnp.where(iota((128, 128), 1) < 64, high.astype(F32), low.astype(F32))
        in_s[half] = spread(inputs[:, half * 128 : (half + 1) * 128])
        rd_s[half] = spread(reads[:, half * 128 : (half + 1) * 128])
        de_s[half] = jnp.broadcast_to(column(decay, half), (128, 128))

    def advance_state(half, low, high):
        lanes = WIDE // 64
        for j in range(low, high):
            in_copy(half, j).wait()
        total = None
        for j in range(low, high):
            here = (slice(None), slice(half * 8, half * 8 + 8), slice(j * WIDE, (j + 1) * WIDE))
            shifted = xs_s[half] if j == 0 else pltpu.roll(xs_s[half], 128 - j * lanes, 1)
            fresh = dot(shifted.astype(BF16), grid[...])
            new = jnp.tile(de_s[half], (1, WIDE // 128)) * new_state[here].reshape(128, WIDE) + fresh * jnp.tile(in_s[half], (1, WIDE // 128))
            new_state[here] = new.reshape(16, 8, WIDE)
            part = dot_t((new * jnp.tile(rd_s[half], (1, WIDE // 128))).astype(BF16), grid[...])
            part = part if j == 0 else pltpu.roll(part, j * lanes, 1)
            total = part if total is None else total + part
        rdo[half] = total if low == 0 else rdo[half] + total

    def finish_state(half):
        keep = (iota((8, 512), 1) // 64) == iota((8, 512), 0)
        wide = jnp.tile(rdo[half], (1, 4)).reshape(16, 8, 512)
        read = jnp.sum(jnp.where(keep[None], wide, 0.0), axis=1)
        gated = read * silu(pz[:, half * 512 : (half + 1) * 512].astype(F32))
        for g in range(2):
            lanes = slice(half * 512 + g * 256, half * 512 + (g + 1) * 256)
            part = gated[:, g * 256 : (g + 1) * 256]
            scale = lax.rsqrt(jnp.mean(part * part, axis=-1, keepdims=True) + EPSILON)
            ybuf[z, :, lanes] = (part * scale * gg[:, lanes]).astype(BF16)

    copies = Copies(ssem)

    def send_y(half):
        ref = ybuf.at[z, :, half * 512 : (half + 1) * 512]
        for zz in zs:
            copies(ref, ref, zsem.at[half, z], z=zz)

    wg = [plane_gather(copies, wbuf, g * 1024, 1024, g, wsem, coords) for g in range(2)]

    def advance(gens):
        for gen in gens:
            next(gen)

    advance_state(0, 0, CHUNKS)
    finish_state(0)
    for load in loads[:5]:
        load.wait()
    pl.semaphore_wait(barrier, 2 * len(zs) + len(sends) + 1)
    send_y(0)
    for yy, xx in sends:
        copies(obuf.at[y, x], obuf.at[y, x], gsem.at[q], y=yy, x=xx)
    advance(wg)
    for load in loads[5:]:
        load.start()
    rbuf[z] = r_ref[:, pl.ds(pl.multiple_of(z * 256 + t * 128, 128), 128)]
    advance_state(1, 0, CHUNKS)
    finish_state(1)
    send_y(1)
    for zz in zs:
        copies(r_ref.at[:, pl.ds(pl.multiple_of(zz * 256 + t * 128, 128), 128)], rbuf.at[z], zsem.at[2, z], z=zz)
    for load in first[EARLY:]:
        load.wait()
    route[...] = jnp.zeros_like(route)
    route[0:6, :] = ids[...].astype(F32)
    route[8:14, :] = ew[...]
    route[16:20, :] = gw[...]
    row, tok = iota((2048, 128), 0), iota((2048, 128), 1)
    take = (row == (tok // 16) * 256 + q * 16 + tok % 16).astype(BF16)
    high, rest = split(route[...])
    mine = dot(high, take) + dot(rest, take)
    expert = iota((16, 128), 0) + z * 16
    hit = jnp.zeros((16, 128), F32)
    weight = jnp.zeros((16, 128), F32)
    for k in range(6):
        same = mine[k : k + 1, :].astype(I32) == expert
        hit = hit + same.astype(F32)
        weight = weight + jnp.where(same, mine[8 + k : 9 + k, :], 0.0)
    coarse = jnp.sum(jnp.where(iota((8, 128), 0) == z // 2, mine[16:24, :], 0.0), axis=0, keepdims=True)
    weight = weight * coarse
    a, b = iota((128, 128), 0), iota((128, 128), 1)
    before = ((a // 16 == b // 16) & (a < b)).astype(BF16)
    rank = dot(hit.astype(BF16), before)
    slot, tok3 = iota((16, 16, 128), 1), iota((16, 16, 128), 2)
    chosen = (
        (hit[:, None, :] > 0.5)
        & (rank[:, None, :] == (slot % 2).astype(F32))
        & (slot // 2 == tok3 // 16)
    )
    disp[...] = jnp.where(chosen, 1.0, 0.0).reshape(256, 128).astype(BF16)
    comb = jnp.where(chosen, jnp.broadcast_to(weight[:, None, :], (16, 16, 128)), 0.0).reshape(256, 128)
    comb = jnp.concatenate([comb[:128].T, comb[128:].T], axis=1)
    high, low = split(comb)
    c_hi[...] = high
    c_lo[...] = low

    for half in range(2):
        for zz in zs[::-1]:
            copies.arrived(ybuf.at[zz, :, half * 512 : (half + 1) * 512], zsem.at[half, zz], z=zz)

    for yy, xx in sends:
        copies.arrived(obuf.at[yy, xx], gsem.at[yy * 4 + xx], y=yy, x=xx)
    rows = ybuf[...].reshape(128, 1024)
    msend[...] = dot_t(rows, obuf[pl.ds(other * 2, 2)].reshape(128, 1024)).astype(BF16)
    copies(msend, mrecv, tsem.at[0], tp=other)
    mown[...] = dot_t(rows, obuf[pl.ds(t * 2, 2)].reshape(128, 1024))
    for zz in zs:
        copies.arrived(rbuf.at[zz], zsem.at[2, zz], z=zz)
    copies.arrived(mrecv, tsem.at[0], tp=other)
    mixed = mown[...] + mrecv[...].astype(F32)
    nbuf[z, t] = (rbuf[...].reshape(128, 128).astype(F32) + mixed).astype(BF16)
    for zz in zs:
        copies(nbuf.at[z, t], nbuf.at[z, t], zsem.at[3, z], z=zz)
    copies(nbuf.at[z, t], nbuf.at[z, t], nsem.at[z], tp=other)
    advance(wg)
    advance(wg)
    advance(wg)
    for i, zz in enumerate(zs):
        copies.arrived(nbuf.at[zz, t], zsem.at[3, zz], z=zz)
        copies(nbuf.at[zz, t], nbuf.at[zz, t], nsem.at[zz], tp=other)
    for load in loads[5:]:
        load.wait()
    for zz in [z] + zs:
        copies.arrived(nbuf.at[zz, other], nsem.at[zz], tp=other)

    for j in range(16):
        rn[:, j * 128 : (j + 1) * 128] = nbuf[j // 2, j % 2]
    wide = rn[...].astype(F32)
    scale = lax.rsqrt(jnp.mean(wide * wide, axis=-1, keepdims=True) + EPSILON)
    normed[...] = (wide * scale * gain[...]).astype(BF16)
    near = pl.ds(pl.multiple_of(t * 1024, 1024), 1024)
    far = pl.ds(pl.multiple_of(other * 1024, 1024), 1024)

    xsend[...] = dot(disp[...], normed[:, near]).astype(BF16).reshape(16, 16, 1024)
    for yy, xx in sends:
        copies(xsend.at[yy * 4 + xx], xfull.at[t, q], asem.at[0, q], y=yy, x=xx)
    xfull[t, q] = xsend[q]
    copies(xsend.at[q], xfull.at[t, q], fsem.at[q], tp=other)

    advance(wg)
    advance(wg)

    def receive(w):
        for yy, xx, self in waves[w]:
            if not self:
                qq = yy * 4 + xx
                copies.arrived(xfull.at[t, qq], asem.at[0, qq], y=yy, x=xx)
                copies(xfull.at[t, qq], xfull.at[t, qq], fsem.at[qq], tp=other)

    def compute(w):
        places = [yy * 4 + xx for yy, xx, _ in waves[w]]
        mine = jnp.concatenate([xfull[t, qq] for qq in places], axis=0)
        gate = dot(mine, eg[near, :])
        lin = dot(mine, eu[near, :])
        for qq in places:
            copies.arrived(xfull.at[other, qq], fsem.at[qq], tp=other)
        theirs = jnp.concatenate([xfull[other, qq] for qq in places], axis=0)
        gate = gate + dot(theirs, eg[far, :])
        lin = lin + dot(theirs, eu[far, :])
        hidden = (silu(gate) * lin).astype(BF16)
        esend[w] = dot(hidden, ed[:, far]).astype(BF16)
        copies(esend.at[w], erecv.at[w], tsem.at[4 + w], tp=other)
        emine[w] = dot(hidden, ed[:, near])

    def send_back(c, yy, xx):
        lanes = pl.ds(c * PART, PART)
        copies(csend.at[yy * 4 + xx, :, lanes], cbuf.at[q, :, lanes], asem.at[1 + c, q], y=yy, x=xx)

    def give_back(w):
        copies.arrived(erecv.at[w], tsem.at[4 + w], tp=other)
        done = (emine[w] + erecv[w].astype(F32)).astype(BF16)
        for i, (yy, xx, self) in enumerate(waves[w]):
            qq = yy * 4 + xx
            if self:
                cbuf[q] = done[i * 16 : (i + 1) * 16]
            else:
                csend[qq] = done[i * 16 : (i + 1) * 16]
                send_back(0, yy, xx)

    receive(0)
    receive(1)
    compute(0)
    compute(1)
    give_back(0)
    give_back(1)
    for c in range(1, PARTS):
        for wave in waves:
            for yy, xx, self in wave:
                if not self:
                    send_back(c, yy, xx)
    advance(wg)
    tokens = normed[...]
    vector = jnp.concatenate([bgate[j : j + 1, :].astype(F32) for j in range(16)], axis=1)
    score = jnp.sum(tokens.astype(F32) * vector, axis=-1, keepdims=True)
    gate = dot_t(tokens, wbuf[:, 0].reshape(256, 2048))
    lin = dot_t(tokens, wbuf[:, 1].reshape(256, 2048))
    hidden = (silu(gate) * lin / (1.0 + jnp.exp(-score))).astype(BF16)
    dsend[...] = dot(hidden, wbuf[:, 2, :, far].reshape(256, 1024)).astype(BF16)
    copies(dsend, drecv, tsem.at[1], tp=other)
    tot[...] = dot(hidden, wbuf[:, 2, :, near].reshape(256, 1024)).reshape(8, 16, 1024)

    copies.arrived(drecv, tsem.at[1], tp=other)
    fin[...] = rn[pl.ds(pl.multiple_of(z * 16, 16), 16), :].astype(F32)
    for c in range(PARTS):
        lanes = slice(c * PART, (c + 1) * PART)
        base = tot[:, :, lanes].reshape(128, PART) + drecv[:, lanes].astype(F32)
        for wave in waves:
            for yy, xx, self in wave:
                if not self:
                    qq = yy * 4 + xx
                    copies.arrived(cbuf.at[qq, :, lanes], asem.at[1 + c, qq], y=yy, x=xx)
        back = cbuf[:, :, lanes].reshape(256, PART)
        total = base + dot(c_hi[...], back) + dot(c_lo[...], back)
        tot[:, :, lanes] = total.reshape(8, 16, PART)
        zsend[c] = total.reshape(8, 2, 8, PART).astype(BF16)
        for zz in zs:
            for tt in (t, other):
                copies(zsend.at[c, zz, tt], zrecv.at[c, z, t], rsem.at[c, z, t], z=zz, tp=tt)
        copies(zsend.at[c, z, other], zrecv.at[c, z, t], rsem.at[c, z, t], tp=other)
    for c in range(PARTS):
        for side in (t, other):
            lanes = pl.ds(pl.multiple_of(side * 1024 + c * PART, PART), PART)
            final = fin[pl.ds(pl.multiple_of(t * 8, 8), 8), lanes]
            if side is t:
                final = final + tot[z, pl.ds(pl.multiple_of(t * 8, 8), 8), c * PART : (c + 1) * PART]
            for zz in zs if side is t else [z] + zs:
                copies.arrived(zrecv.at[c, zz, side], rsem.at[c, zz, side], tp=other)
                final = final + zrecv[c, zz, side].astype(F32)
            out_ref[:, lanes] = final.astype(BF16)
    copies.drain()


def shards(resid, proj_x, proj_z, proj_bc, proj_dt, tail_x, tail_bc, taps_x, taps_bc, ssm_state, dt_bias, decay_log,
           group_gain, out_proj, ffn_gain, dense_gate, dense_up, dense_down, branch_gate, group_weights, expert_ids,
           expert_weights, exp_gate, exp_up, exp_down):
    small = (proj_x, proj_z, proj_bc, proj_dt, tail_x.transpose(1, 0, 2), tail_bc, taps_x, taps_bc, dt_bias.reshape(1, 16),
             decay_log.reshape(1, 16), group_gain.reshape(1, 1024), expert_ids.T, expert_weights.T, group_weights.T)
    vm = pl.BlockSpec(memory_space=VMEM)
    hbm = pl.BlockSpec(memory_space=pltpu.MemorySpace.HBM)
    scratch = [pltpu.VMEM(a.shape, a.dtype) for a in small]
    for shape, dtype in (
        ((32, 2048), F32), ((128, WIDE), BF16), ((2, 128, 128), F32), ((2, 128, 128), F32), ((2, 128, 128), F32),
        ((2, 128, 128), F32), ((2, 128, 128), F32), ((256, 128), BF16), ((128, 256), BF16), ((128, 256), BF16),
        ((16, 2048), BF16), ((1, 2048), F32), ((16, 128), BF16),
        ((16, 3, 16, 2048), BF16), ((4, 4, 16, 1024), BF16), ((8, 16, 1024), BF16), ((8, 16, 128), BF16),
        ((128, 128), F32), ((128, 128), BF16), ((128, 128), BF16), ((8, 2, 128, 128), BF16), ((128, 2048), BF16),
        ((128, 2048), BF16), ((128, 1024), BF16), ((128, 1024), BF16), ((16, 16, 1024), BF16), ((2, 16, 16, 1024), BF16),
        ((2, 128, 1024), F32), ((2, 128, 1024), BF16), ((2, 128, 1024), BF16), ((16, 16, 1024), BF16), ((16, 16, 1024), BF16),
        ((8, 16, 1024), F32), ((PARTS, 8, 2, 8, PART), BF16), ((PARTS, 8, 2, 8, PART), BF16), ((16, 2048), F32),
        ((2048, 256), BF16), ((2048, 256), BF16), ((256, 2048), BF16),
    ):
        scratch.append(pltpu.VMEM(shape, dtype))
    for shape in ((160 + 45 * PARTS,), (2, 16, 2), (16,), (4, 8), (1 + PARTS, 16), (8,), (8,), (16,), (PARTS, 8, 2), (10,), (SMALL,), (2, CHUNKS)):
        scratch.append(pltpu.SemaphoreType.DMA(shape))
    new_state, out = pl.pallas_call(
        mesh_kernel,
        out_shape=(VMEM((16, 16, 4096), F32), VMEM((8, 2048), BF16)),
        in_specs=[hbm] * (SMALL + 11),
        out_specs=(vm, vm),
        scratch_shapes=scratch,
        compiler_params=pltpu.CompilerParams(collective_id=0, has_side_effects=True, vmem_limit_bytes=67_043_328 - (4200 << 10)),
        name="mesh",
    )(*small, ssm_state, resid, out_proj.T, dense_gate.T, dense_up.T, dense_down, ffn_gain.reshape(1, 2048),
      branch_gate.reshape(16, 128), exp_gate, exp_up, exp_down)
    return (out, new_state)


def solution(mesh):
    finer = Mesh(mesh.devices.reshape(NZ, NY, NX, mesh.shape["tp"]), EP_TP)
    in_specs = (
        P(EP, None), P(EP, "tp"), P(EP, "tp"), P(EP, None, "tp"), P(EP, "tp"), P(EP, None, "tp"), P(EP, None, None, "tp"),
        P(None, "tp"), P(None, None, "tp"), P(EP, "tp", None), P("tp"), P("tp"), P("tp"), P("tp", EP), P(),
        P(None, EP_TP), P(None, EP_TP), P(EP_TP, None), P(), P(), P(), P(), P(EP, None, "tp"), P(EP, None, "tp"),
        P(EP, "tp", None),
    )
    out_specs = (P(EP_TP, None), P(EP, "tp", None))
    return jax.shard_map(shards, mesh=finer, in_specs=in_specs, out_specs=out_specs, check_vma=False)
```
